32 devices in a mesh: sp: 8 (over z, x), tp: 4 (over y, core).
Axes of the slice: x: 2, y: 2, z: 4, core: 2. Of those that a mesh axis runs over, the one named last changes fastest.
Arguments:
- tokens: bfloat16 [2048, 2048], P('sp', 'tp'), may hold values from -6 to 6
- norm_gain: float32 [2048], replicated, may hold values from 0.1 to 1.9
- query_one: bfloat16 [2048, 512], P('sp', 'tp'), may hold values from -1 to 1
- key_one: bfloat16 [2048, 512], P('sp', 'tp'), may hold values from -1 to 1
- query_two: bfloat16 [2048, 512], P('sp', 'tp'), may hold values from -0.15625 to 0.15625
- key_two: bfloat16 [2048, 512], P('sp', 'tp'), may hold values from -0.15625 to 0.15625
- value_weight: bfloat16 [2048, 1024], P('sp', 'tp'), may hold values from -0.5 to 0.5
- pool_weight: bfloat16 [2048, 1024], P('sp', 'tp'), may hold values from -0.125 to 0.125
- lambda_head: float32 [8], replicated, may hold values from 0.3 to 0.8
- head_gain: float32 [128], replicated, may hold values from 0.1 to 1.9
- group_weight: bfloat16 [8, 128, 128], replicated, may hold values from -0.5 to 0.5
- pool_scale: float32 [1024], replicated, may hold values from 0.1 to 1.9
- out_attn: bfloat16 [1024, 2048], P('tp', 'sp'), may hold values from -0.125 to 0.125
- out_pool: bfloat16 [1024, 2048], P('tp', 'sp'), may hold values from -0.125 to 0.125
Outputs:
- mixed: bfloat16 [2048, 2048], P(('sp', 'tp'))
The draws below stay inside these ranges and needn't reach their ends.
All inputs are finite; a program needn't handle non-finite values.
Results may differ from the reference program's by a relative error of at most 0.013.
Values may be sent and summed in bfloat16 or wider, within the bound.
A program may use at most 128 MiB of HBM per device.

```python
import math
import jax
import jax.numpy as jnp
from jax import lax

D = 2048
HEADS = 8
HEAD_DIM = 64
VALUE_DIM = 128
GROUPS = 8
GROUP_DIM = 128
TOKENS = 2048


def paired_weights(key):
    first_draw = jax.random.normal(jax.random.fold_in(key, 101), (D, HEADS * HEAD_DIM), jnp.float32)
    second_draw = jax.random.normal(jax.random.fold_in(key, 202), (D, HEADS * HEAD_DIM), jnp.float32)
    query_part = jnp.clip(first_draw, -4.0, 4.0) * (1.3 / jnp.sqrt(jnp.float32(D)))
    key_part = jnp.clip(second_draw, -4.0, 4.0) * (1.3 / jnp.sqrt(jnp.float32(D)))
    return (query_part, key_part)


def draw_query_one(key, part):
    return paired_weights(key)[0].astype(jnp.bfloat16)


def draw_key_one(key, part):
    return paired_weights(key)[1].astype(jnp.bfloat16)


def levels(rng, shape, shards, smallest, high):
    gain = 1.0
    for position, blocks in shards:
        steps = jax.random.uniform(jax.random.fold_in(jax.random.fold_in(rng, 6), position), (blocks,), jnp.float32, smallest / len(shards), high / len(shards))
        gain = gain * jnp.repeat(jnp.exp(steps), shape[position] // blocks).reshape((-1,) + (1,) * (len(shape) - 1 - position))
    return gain


def normal_values(key, extent, spread, limit, split=(), held_as=jnp.bfloat16):
    loudness = levels(key, extent, split, -0.22, 0.18) if split else 1.0
    array = jax.random.normal(key, extent, jnp.float32) * spread * loudness
    return jnp.minimum(jnp.maximum(array, -limit), limit).astype(held_as)


def setup_inputs(seed: int = 0) -> dict:
    arg_keys = jax.random.split(jax.random.key(seed), 15)
    return {
        "tokens": normal_values(arg_keys[0], (TOKENS, D), 1.0, 6.0, ((0, 8), (1, 4))),
        "norm_gain": jnp.clip(1.0 + 0.18 * jax.random.normal(arg_keys[1], (D,), jnp.float32), 0.1, 1.9),
        "query_one": draw_query_one(jax.random.fold_in(arg_keys[14], 71), 0),
        "key_one": draw_key_one(jax.random.fold_in(arg_keys[14], 71), 0),
        "query_two": normal_values(arg_keys[4], (D, HEADS * HEAD_DIM), (D * 100 // 169) ** -0.5, 0.15625, ((0, 8), (1, 4))),
        "key_two": normal_values(arg_keys[5], (D, HEADS * HEAD_DIM), (D * 100 // 169) ** -0.5, 0.15625, ((0, 8), (1, 4))),
        "value_weight": normal_values(arg_keys[6], (D, HEADS * VALUE_DIM), (D // 16) ** -0.5, 0.5, ((0, 8), (1, 4))),
        "pool_weight": normal_values(arg_keys[7], (D, GROUPS * GROUP_DIM), D ** -0.5, 0.125, ((0, 8), (1, 4))),
        "lambda_head": jnp.clip(jax.random.uniform(arg_keys[8], (HEADS,), jnp.float32, 0.3, 0.8), 0.3, 0.8),
        "head_gain": jnp.clip(1.0 + 0.18 * jax.random.normal(arg_keys[9], (VALUE_DIM,), jnp.float32), 0.1, 1.9),
        "group_weight": normal_values(arg_keys[10], (GROUPS, GROUP_DIM, GROUP_DIM), GROUP_DIM ** -0.5, 0.5),
        "pool_scale": jnp.clip(1.0 + 0.18 * jax.random.normal(arg_keys[11], (GROUPS * GROUP_DIM,), jnp.float32), 0.1, 1.9),
        "out_attn": normal_values(arg_keys[12], (HEADS * VALUE_DIM, D), (HEADS * VALUE_DIM + GROUPS * GROUP_DIM) ** -0.5, 0.125, ((0, 4), (1, 8))),
        "out_pool": normal_values(arg_keys[13], (GROUPS * GROUP_DIM, D), (HEADS * VALUE_DIM + GROUPS * GROUP_DIM) ** -0.5, 0.125, ((0, 4), (1, 8))),
    }


rope_base = 500000.0
head_scale = 0.8
norm_floor = 1e-06
head_floor = 0.001
masked_score = -1e+30

def rotate(values_in, positions):
    half_dim = values_in.shape[-1] // 2
    inverse = rope_base ** (-(jnp.arange(half_dim, dtype=jnp.float32) * 2.0 / values_in.shape[-1]))
    angles = positions.astype(jnp.float32)[:, None] * inverse[None, :]
    cosine = jnp.cos(angles)[:, None, :]
    sine_part = jnp.sin(angles)[:, None, :]
    first_half = values_in[..., :half_dim]
    second_half = values_in[..., half_dim:]
    return jnp.concatenate([first_half * cosine - second_half * sine_part, second_half * cosine + first_half * sine_part], axis=-1)

def reference(tokens, norm_gain, query_one, key_one, query_two, key_two, value_weight, pool_weight, lambda_head, head_gain, group_weight, pool_scale, out_attn, out_pool):
    float_rows = tokens.astype(jnp.float32)
    normed = (float_rows * lax.rsqrt(lax.optimization_barrier(jnp.mean(float_rows * float_rows, axis=-1, keepdims=True)) + norm_floor) * norm_gain).astype(jnp.bfloat16)
    positions = jnp.arange(TOKENS, dtype=jnp.int32)
    score_scale = HEAD_DIM ** (-0.5)

    def project(weight):
        return jnp.dot(normed, weight, preferred_element_type=jnp.float32)

    def turned(weight):
        rounded_rows = rotate(project(weight).reshape(TOKENS, HEADS, HEAD_DIM), positions).astype(jnp.bfloat16)
        return lax.optimization_barrier(rounded_rows).astype(jnp.float32)
    query_a = turned(query_one)
    key_a = turned(key_one)
    query_b = turned(query_two)
    key_b = turned(key_two)
    value_rows = lax.optimization_barrier(project(value_weight).astype(jnp.bfloat16)).astype(jnp.float32).reshape(TOKENS, HEADS, VALUE_DIM)
    query_block = math.gcd(TOKENS, 256)
    blocks = TOKENS // query_block

    def one_block(block_id):
        start_row = block_id * query_block
        query_pos = start_row + jnp.arange(query_block, dtype=jnp.int32)
        visible = (positions[None, :] <= query_pos[:, None])[:, None, :]
        map_means = []
        for query_all, key_all in ((query_a, key_a), (query_b, key_b)):
            query_part = lax.dynamic_slice_in_dim(query_all, start_row, query_block, 0)
            scores = jnp.einsum('qhd,khd->qhk', query_part, key_all) * score_scale
            scores = jnp.where(visible, scores, masked_score)
            top_row = lax.optimization_barrier(jnp.max(scores, axis=-1, keepdims=True))
            weights = jnp.where(visible, jnp.exp(scores - top_row), 0.0)
            totals = lax.optimization_barrier(jnp.sum(weights, axis=-1))
            rounded = lax.optimization_barrier(weights.astype(jnp.bfloat16)).astype(jnp.float32)
            map_means.append(jnp.einsum('qhk,khd->qhd', rounded, value_rows) / totals[..., None])
        differed = map_means[0] - lambda_head[None, :, None] * map_means[1]
        scaled = differed * lax.rsqrt(lax.optimization_barrier(jnp.mean(differed * differed, axis=-1, keepdims=True)) + head_floor) * head_gain * head_scale
        return scaled.astype(jnp.bfloat16)
    attn_out = lax.map(one_block, jnp.arange(blocks, dtype=jnp.int32)).reshape(TOKENS, HEADS * VALUE_DIM)
    pool_rows = lax.optimization_barrier(project(pool_weight).astype(jnp.bfloat16)).astype(jnp.float32)
    running = jnp.cumsum(pool_rows, axis=0)
    results = []
    for group_id in range(GROUPS):
        window = 2 ** (group_id % 4 + 1)
        first_col = group_id * GROUP_DIM
        section = running[:, first_col:first_col + GROUP_DIM]
        earlier = jnp.pad(section, ((window, 0), (0, 0)))[:TOKENS]
        counts = jnp.minimum(positions + 1, window).astype(jnp.float32)
        window_mean = (section - earlier) / counts[:, None] - pool_rows[:, first_col:first_col + GROUP_DIM]
        results.append(jnp.dot(window_mean.astype(jnp.bfloat16), group_weight[group_id], preferred_element_type=jnp.float32))
    pooled = (jnp.concatenate(results, axis=1) * pool_scale).astype(jnp.bfloat16)
    mixed = jnp.dot(attn_out, out_attn, preferred_element_type=jnp.float32) + jnp.dot(pooled, out_pool, preferred_element_type=jnp.float32)
    return mixed.astype(jnp.bfloat16)
```

```python
import functools

import jax
import jax.numpy as jnp
from jax import lax
from jax.experimental import pallas as pl
from jax.experimental.pallas import tpu as pltpu
from jax.sharding import PartitionSpec as P

HEAD_DIM = 64
VALUE_DIM = 128
GROUP_DIM = 128
ROPE_BASE = 500000.0
HEAD_SCALE = 0.8
NORM_FLOOR = 1e-06
HEAD_FLOOR = 0.001
MASKED = -1e30
TAIL = 16
HALVES = 2
MESH = pl.DeviceIdType.MESH
BF16 = jnp.bfloat16
F32 = jnp.float32


def flip(index, bit):
    return index + bit * (1 - 2 * ((index // bit) % 2))


def kernel(
    sizes,
    tok_ref,
    gain_ref,
    wp_ref,
    op_ref,
    cos_ref,
    sin_ref,
    lam_ref,
    hg_ref,
    gw_ref,
    ps_ref,
    out_ref,
    tokbuf,
    nrm,
    w_all,
    o_all,
    kv,
    q_st,
    m_st,
    l_st,
    acc_st,
    pool,
    tail,
    prior,
    cat,
    part,
    sbuf,
    rbuf,
    tok_send,
    tok_recv,
    w_up,
    w_dn,
    w_recv,
    wx_send,
    o_up,
    o_dn,
    o_recv,
    ox_send,
    kv_send,
    kv_recv,
    pp_send,
    pp_recv,
    rs_send,
    rs_recv,
):
    G, R, TP = sizes
    s = lax.axis_index("sp")
    t = lax.axis_index("tp")
    r = s // G
    g = s % G
    head = t * G + g
    other = s + 1 - 2 * g
    chunk, feats = tok_ref.shape
    rows = G * chunk
    has_up = r + 1 < R
    has_dn = r > 0

    t_bits = []
    bit = 1
    while bit < TP:
        t_bits.append(("t", bit))
        bit *= 2
    x_dim = ("g", 1)
    members = G * TP

    def member(mask):
        gg, tt = g, t
        for kind, b in mask:
            if kind == "g":
                gg = flip(gg, b)
            else:
                tt = flip(tt, b)
        return gg, tt

    def device(mask):
        gg, tt = member(mask)
        return (r * G + gg, tt)

    barrier = pltpu.get_barrier_semaphore()
    for dim in [x_dim] + t_bits:
        pl.semaphore_signal(barrier, inc=1, device_id=device([dim]), device_id_type=MESH)

    @pl.when(has_up)
    def _():
        pl.semaphore_signal(barrier, inc=1, device_id=(s + G, t), device_id_type=MESH)

    @pl.when(has_dn)
    def _():
        pl.semaphore_signal(barrier, inc=1, device_id=(s - G, t), device_id_type=MESH)

    count = 1 + len(t_bits) + jnp.where(has_up, 1, 0) + jnp.where(has_dn, 1, 0)
    pl.semaphore_wait(barrier, count)

    def rdma(src, dst, ss, rs, dev):
        return pltpu.make_async_remote_copy(
            src_ref=src, dst_ref=dst, send_sem=ss, recv_sem=rs, device_id=dev, device_id_type=MESH
        )

    def up_copy(src, buf, k, up, recv):
        return rdma(src, buf.at[k], up.at[k], recv.at[k], (s + G, t))

    def dn_copy(src, buf, k, dn, recv):
        return rdma(src, buf.at[k], dn.at[k], recv.at[k], (s - G, t))

    def send_both(src, buf, k, up, dn, recv):
        @pl.when(has_up)
        def _():
            up_copy(src, buf, k, up, recv).start()

        @pl.when(has_dn)
        def _():
            dn_copy(src, buf, k, dn, recv).start()

    def cross_copy(inp, buf, xs, recv):
        return rdma(inp.at[1 - g], buf.at[s], xs, recv.at[s], (other, t))

    def wait_slot(buf, k, up, recv):
        up_copy(buf.at[k], buf, k, up, recv).wait_recv()

    def line_step(j, buf, up, dn, recv):
        for gg in (g, 1 - g):
            @pl.when(r - 1 - j >= 0)
            def _():
                k = (r - 1 - j) * G + gg
                wait_slot(buf, k, up, recv)

                @pl.when(has_up)
                def _():
                    up_copy(buf.at[k], buf, k, up, recv).start()

            @pl.when(r + 1 + j < R)
            def _():
                k = (r + 1 + j) * G + gg
                wait_slot(buf, k, up, recv)

                @pl.when(has_dn)
                def _():
                    dn_copy(buf.at[k], buf, k, dn, recv).start()

    def drain(buf, up, dn, recv):
        @pl.when(has_up)
        def _():
            @pl.loop(0, (r + 1) * G)
            def _(k):
                up_copy(buf.at[k], buf, k, up, recv).wait_send()

        @pl.when(has_dn)
        def _():
            @pl.loop(r * G, R * G)
            def _(k):
                dn_copy(buf.at[k], buf, k, dn, recv).wait_send()

    tok_dims = t_bits[1:] + [x_dim] + t_bits[:1]
    tok_stages = []
    held = [[]]
    slot = 0
    for dim in tok_dims:
        stage = []
        for mask in held:
            gg, tt = member(mask)
            src = tok_ref if not mask else tokbuf.at[gg, tt]
            stage.append((mask, src, slot))
            slot += 1
        tok_stages.append((dim, stage))
        held = held + [mask + [dim] for mask in held]

    def tok_copy(dim, mask, src, index):
        gg, tt = member(mask)
        return rdma(src, tokbuf.at[gg, tt], tok_send.at[index], tok_recv.at[index], device([dim]))

    def tok_start(i):
        dim, stage = tok_stages[i]
        for mask, src, index in stage:
            tok_copy(dim, mask, src, index).start()

    def tok_wait(i):
        dim, stage = tok_stages[i]
        for mask, src, index in stage:
            gg, tt = member(mask + [dim])
            rdma(
                tokbuf.at[gg, tt], tokbuf.at[gg, tt], tok_send.at[index], tok_recv.at[index],
                device([dim]),
            ).wait_recv()

    send_both(wp_ref.at[g], w_all, s, w_up, w_dn, w_recv)
    cross_copy(wp_ref, w_all, wx_send, w_recv).start()
    tok_start(0)
    w_all[s] = wp_ref[g]
    o_all[s] = op_ref[g]
    tokbuf[g, t] = tok_ref[...]
    wait_slot(w_all, other, w_up, w_recv)
    send_both(w_all.at[other], w_all, other, w_up, w_dn, w_recv)
    stage_count = len(tok_stages)
    tok_wait(0)
    tok_start(1)
    cross_copy(op_ref, o_all, ox_send, o_recv).start()
    line_step(0, w_all, w_up, w_dn, w_recv)
    for i in range(1, stage_count):
        tok_wait(i)
        if i + 1 < stage_count:
            tok_start(i + 1)
            if i < R - 1:
                line_step(i, w_all, w_up, w_dn, w_recv)
    done_steps = min(stage_count - 1, R - 1)

    gain = gain_ref[...]
    tile = chunk // 2

    @pl.loop(0, G * 2)
    def _(b):
        gi = b // 2
        off = pl.multiple_of((b % 2) * tile, tile)
        dst = pl.multiple_of(b * tile, tile)
        total = jnp.zeros((tile, 1), F32)
        for i in range(TP):
            x = tokbuf[gi, i, pl.ds(off, tile), :].astype(F32)
            total = total + jnp.sum(x * x, axis=-1, keepdims=True)
        inv = lax.rsqrt(total / (TP * feats) + NORM_FLOOR)
        for i in range(TP):
            x = tokbuf[gi, i, pl.ds(off, tile), :].astype(F32)
            nrm[pl.ds(dst, tile), i * feats : (i + 1) * feats] = (
                x * inv * gain[:, i * feats : (i + 1) * feats]
            ).astype(BF16)

    if done_steps < R - 1:
        @pl.loop(done_steps, R - 1)
        def _(j):
            line_step(j, w_all, w_up, w_dn, w_recv)

    send_both(op_ref.at[g], o_all, s, o_up, o_dn, o_recv)
    wait_slot(o_all, other, o_up, o_recv)
    send_both(o_all.at[other], o_all, other, o_up, o_dn, o_recv)

    width = wp_ref.shape[2]
    ptile = chunk

    def rope(x, cosine, sine):
        lane = lax.broadcasted_iota(jnp.int32, x.shape, 1)
        near = jnp.where(
            lane % HEAD_DIM < HEAD_DIM // 2,
            pltpu.roll(x, x.shape[1] - HEAD_DIM // 2, 1),
            pltpu.roll(x, HEAD_DIM // 2, 1),
        )
        return x * cosine + near * sine

    @pl.loop(0, rows // ptile)
    def _(b):
        at = pl.ds(pl.multiple_of(b * ptile, ptile), ptile)
        weights = w_all[...].reshape(-1, width)
        y = jnp.dot(nrm[at, :], weights, preferred_element_type=F32)
        cosine = cos_ref[at, :]
        sine = sin_ref[at, :]
        kv[r, at, 0:128] = rope(y[:, 128:256], cosine, sine).astype(BF16)
        kv[r, at, 128:256] = y[:, 256:384].astype(BF16)
        p = y[:, 384:512].astype(BF16)
        pool[pl.ds(pl.multiple_of(TAIL + b * ptile, TAIL), ptile), :] = p.astype(F32)
        tail[...] = p[ptile - TAIL :, :]
        q = rope(y[:, 0:128], cosine, sine).astype(BF16) * jnp.array(HEAD_DIM**-0.5, BF16)
        lane = lax.broadcasted_iota(jnp.int32, q.shape, 1)
        zero = jnp.zeros_like(q)
        q_st[0, at, :] = jnp.where(lane < HEAD_DIM, q, zero)
        q_st[1, at, :] = jnp.where(lane >= HEAD_DIM, q, zero)

    def kv_copy(k):
        return rdma(kv.at[k], kv.at[k], kv_send.at[k], kv_recv.at[k], (s + G, t))

    tail_copy = rdma(tail, prior, pp_send, pp_recv, (s + G, t))

    @pl.when(has_up)
    def _():
        kv_copy(r).start()
        tail_copy.start()

    qtile = rows // 2

    def attend(k, diagonal):
        @pl.loop(0, 4)
        def _(b):
            m_index = b // 2
            at = pl.ds(pl.multiple_of((b % 2) * qtile, qtile), qtile)
            q = q_st[m_index, at, :]
            scores = lax.dot_general(
                q, kv[k, :, 0:128], (((1,), (1,)), ((), ())), preferred_element_type=F32
            )
            if diagonal:
                qpos = (b % 2) * qtile + lax.broadcasted_iota(jnp.int32, scores.shape, 0)
                kpos = lax.broadcasted_iota(jnp.int32, scores.shape, 1)
                scores = jnp.where(kpos <= qpos, scores, MASKED)
            top = jnp.max(scores, axis=-1, keepdims=True)
            if not diagonal:
                old = m_st[m_index, at, :]
                top = jnp.maximum(old, top)
                factor = jnp.exp(old - top)
            weights = jnp.exp(scores - top)
            total = jnp.sum(weights, axis=-1, keepdims=True)
            product = jnp.dot(weights.astype(BF16), kv[k, :, 128:256], preferred_element_type=F32)
            if not diagonal:
                total = total + l_st[m_index, at, :] * factor
                product = product + acc_st[m_index, at, :] * factor
            m_st[m_index, at, :] = top
            l_st[m_index, at, :] = total
            acc_st[m_index, at, :] = product

    attend(r, True)

    @pl.loop(0, R - 1)
    def _(j):
        line_step(j, o_all, o_up, o_dn, o_recv)

        @pl.when(j < r)
        def _():
            k = r - 1 - j
            kv_copy(k).wait_recv()

            @pl.when(has_up)
            def _():
                kv_copy(k).start()

            attend(k, False)

    @pl.when(has_dn)
    def _():
        tail_copy.wait_recv()
        pool[0:TAIL, :] = prior[...].astype(F32)

    @pl.when(r == 0)
    def _():
        pool[0:TAIL, :] = jnp.zeros((TAIL, GROUP_DIM), F32)

    ext = pool[...]
    kind = head % 4
    window = jnp.where(kind == 0, 2, jnp.where(kind == 1, 4, jnp.where(kind == 2, 8, 16)))
    run = ext + pltpu.roll(ext, 1, 0)
    chosen = run
    for power, lag in ((1, 2), (2, 4), (3, 8)):
        run = run + pltpu.roll(run, lag, 0)
        chosen = jnp.where(kind == power, run, chosen)
    spot = r * rows + lax.broadcasted_iota(jnp.int32, (rows, GROUP_DIM), 0)
    counts = jnp.minimum(spot + 1, window).astype(F32)
    mean = chosen[TAIL:, :] / counts - ext[TAIL:, :]
    mixedg = jnp.dot(mean.astype(BF16), gw_ref[head], preferred_element_type=F32)
    cat[:, 128:256] = (mixedg * ps_ref[head]).astype(BF16)

    diff = acc_st[0] / l_st[0] - lam_ref[head] * (acc_st[1] / l_st[1])
    inv = lax.rsqrt(jnp.mean(diff * diff, axis=-1, keepdims=True) + HEAD_FLOOR)
    cat[:, 0:128] = (diff * inv * hg_ref[...] * HEAD_SCALE).astype(BF16)

    share = rows // members
    o_rows = o_all.shape[0] * o_all.shape[1]
    half = o_rows // HALVES
    o_slots = o_all.shape[0] // HALVES
    orders = ([t_bits[0], x_dim] + t_bits[1:], t_bits + [x_dim])

    def block(mask):
        gg, tt = member(mask)
        return pl.ds(pl.multiple_of((gg * TP + tt) * share, share), share)

    def combos(dims):
        found = [[]]
        for dim in dims:
            found = found + [mask + [dim] for mask in found]
        return found

    plans = []
    for h in range(HALVES):
        order = orders[h % 2]
        stages = []
        base = 0
        for i, dim in enumerate(order):
            masks = combos(order[i + 1 :])
            stages.append((dim, masks, base))
            base += len(masks)
        plans.append(stages)

    def rs_copy(h, dim, mask, index):
        at = block([dim] + mask)
        return rdma(
            sbuf.at[h, at, :], rbuf.at[h, index], rs_send.at[h, index], rs_recv.at[h, index],
            device([dim]),
        )

    def rs_start(h, i):
        dim, masks, base = plans[h][i]
        for n, mask in enumerate(masks):
            at = block([dim] + mask)
            sbuf[h, at, :] = part[h, at, :].astype(BF16)
        for n, mask in enumerate(masks):
            rs_copy(h, dim, mask, base + n).start()

    def rs_finish(h, i):
        dim, masks, base = plans[h][i]
        for n, mask in enumerate(masks):
            rs_copy(h, dim, mask, base + n).wait_recv()
            at = block(mask)
            part[h, at, :] = part[h, at, :] + rbuf[h, base + n].astype(F32)

    for h in range(HALVES):
        @pl.loop(0, 4)
        def _(b):
            at = pl.ds(pl.multiple_of(b * (rows // 4), rows // 4), rows // 4)
            columns = o_all[h * o_slots : (h + 1) * o_slots].reshape(half, -1)
            part[h, at, :] = lax.dot_general(
                cat[at, :], columns, (((1,), (1,)), ((), ())), preferred_element_type=F32
            )

        rs_start(h, 0)

    levels = len(plans[0])
    for i in range(levels):
        for h in range(HALVES):
            rs_finish(h, i)
            if i + 1 < levels:
                rs_start(h, i + 1)
    mine = block([])
    for h in range(HALVES):
        out_ref[:, h * half : (h + 1) * half] = part[h, mine, :].astype(BF16)

    cross_copy(wp_ref, w_all, wx_send, w_recv).wait_send()
    cross_copy(op_ref, o_all, ox_send, o_recv).wait_send()
    drain(w_all, w_up, w_dn, w_recv)
    drain(o_all, o_up, o_dn, o_recv)
    for dim, stage in tok_stages:
        for mask, src, index in stage:
            tok_copy(dim, mask, src, index).wait_send()

    @pl.when(has_up)
    def _():
        tail_copy.wait_send()

        @pl.loop(0, r + 1)
        def _(k):
            kv_copy(k).wait_send()

    for h in range(HALVES):
        for dim, masks, base in plans[h]:
            for n, mask in enumerate(masks):
                rs_copy(h, dim, mask, base + n).wait_send()


def body(
    sp,
    tp,
    tokens,
    norm_gain,
    query_one,
    key_one,
    query_two,
    key_two,
    value_weight,
    pool_weight,
    lambda_head,
    head_gain,
    group_weight,
    pool_scale,
    out_attn,
    out_pool,
):
    G = query_one.shape[1] // HEAD_DIM
    assert G == 2 and sp % G == 0
    R = sp // G
    chunk, feats = tokens.shape
    rows = G * chunk
    depth = query_one.shape[0]
    cols = out_attn.shape[1]
    heads = lambda_head.shape[0]
    members = G * tp
    share = rows // members

    def heads_first(w):
        return w.reshape(depth, G, -1)

    packed = jnp.concatenate(
        [
            heads_first(w)
            for w in (query_one, query_two, key_one, key_two, value_weight, pool_weight)
        ],
        axis=2,
    ).transpose(1, 0, 2)
    out_packed = jnp.concatenate(
        [out_attn.reshape(G, VALUE_DIM, cols), out_pool.reshape(G, GROUP_DIM, cols)], axis=1
    ).transpose(0, 2, 1)

    line = lax.axis_index("sp") // G
    half_dim = HEAD_DIM // 2
    lane = jnp.arange(2 * HEAD_DIM, dtype=jnp.int32)
    inverse = ROPE_BASE ** (-((lane % half_dim).astype(F32) * 2.0 / HEAD_DIM))
    positions = line * rows + jnp.arange(rows, dtype=jnp.int32)
    angles = positions.astype(F32)[:, None] * inverse[None, :]
    cosine = jnp.cos(angles)
    sine = jnp.where(lane % HEAD_DIM < half_dim, -1.0, 1.0)[None, :] * jnp.sin(angles)

    width = packed.shape[2]
    depth_out = out_packed.shape[2]
    total_cols = sp * cols
    vm = pl.BlockSpec(memory_space=pltpu.VMEM)
    dma = pltpu.SemaphoreType.DMA
    return pl.pallas_call(
        functools.partial(kernel, (G, R, tp)),
        out_shape=jax.ShapeDtypeStruct((share, total_cols), BF16),
        in_specs=[vm] * 6 + [pl.BlockSpec(memory_space=pltpu.SMEM)] + [vm] * 3,
        out_specs=vm,
        scratch_shapes=[
            pltpu.VMEM((G, tp, chunk, feats), BF16),
            pltpu.VMEM((rows, tp * feats), BF16),
            pltpu.VMEM((sp, depth, width), BF16),
            pltpu.VMEM((sp, cols, depth_out), BF16),
            pltpu.VMEM((R, rows, 256), BF16),
            pltpu.VMEM((2, rows, 128), BF16),
            pltpu.VMEM((2, rows, 1), F32),
            pltpu.VMEM((2, rows, 1), F32),
            pltpu.VMEM((2, rows, VALUE_DIM), F32),
            pltpu.VMEM((TAIL + rows, GROUP_DIM), F32),
            pltpu.VMEM((TAIL, GROUP_DIM), BF16),
            pltpu.VMEM((TAIL, GROUP_DIM), BF16),
            pltpu.VMEM((rows, depth_out), BF16),
            pltpu.VMEM((HALVES, rows, total_cols // HALVES), F32),
            pltpu.VMEM((HALVES, rows, total_cols // HALVES), BF16),
            pltpu.VMEM((HALVES, members - 1, share, total_cols // HALVES), BF16),
            dma((members - 1,)),
            dma((members - 1,)),
            dma((sp,)),
            dma((sp,)),
            dma((sp,)),
            dma,
            dma((sp,)),
            dma((sp,)),
            dma((sp,)),
            dma,
            dma((R,)),
            dma((R,)),
            dma,
            dma,
            dma((HALVES, members - 1)),
            dma((HALVES, members - 1)),
        ],
        compiler_params=pltpu.CompilerParams(
            collective_id=0, has_side_effects=True, vmem_limit_bytes=58 * 1024 * 1024
        ),
    )(
        tokens,
        norm_gain.reshape(1, -1),
        packed,
        out_packed,
        cosine,
        sine,
        lambda_head,
        head_gain.reshape(1, -1),
        group_weight,
        pool_scale.reshape(heads, 1, GROUP_DIM),
    )


def solution(mesh):
    in_specs = (
        P("sp", "tp"),
        P(),
        P("sp", "tp"),
        P("sp", "tp"),
        P("sp", "tp"),
        P("sp", "tp"),
        P("sp", "tp"),
        P("sp", "tp"),
        P(),
        P(),
        P(),
        P(),
        P("tp", "sp"),
        P("tp", "sp"),
    )
    return jax.shard_map(
        functools.partial(body, mesh.shape["sp"], mesh.shape["tp"]),
        mesh=mesh,
        in_specs=in_specs,
        out_specs=P(("sp", "tp"), None),
        check_vma=False,
    )
```

```python
import functools

import jax
import jax.numpy as jnp
import numpy as np
from jax import lax
from jax.experimental import pallas as pl
from jax.experimental.pallas import tpu as pltpu
from jax.sharding import PartitionSpec as P

HEAD_DIM = 64
VALUE_DIM = 128
GROUP_DIM = 128
ROPE_BASE = 500000.0
HEAD_SCALE = 0.8
NORM_FLOOR = 1e-06
HEAD_FLOOR = 0.001
MASKED = -1e30
TAIL = 16
CHUNKS = 4
MESH = pl.DeviceIdType.MESH
BF16 = jnp.bfloat16
F32 = jnp.float32


def flip(index, bit):
    return index + bit * (1 - 2 * ((index // bit) % 2))


def kernel(
    sizes,
    tok_ref,
    gain_ref,
    q1_ref,
    k1_ref,
    q2_ref,
    k2_ref,
    v_ref,
    p_ref,
    oa_ref,
    ob_ref,
    freq_ref,
    lam_ref,
    hg_ref,
    gw_ref,
    ps_ref,
    out_ref,
    wp_ref,
    op_ref,
    cos_ref,
    sin_ref,
    yacc,
    tokbuf,
    nrm,
    w_all,
    o_all,
    kv,
    q_st,
    m_st,
    l_st,
    acc_st,
    pool,
    tail,
    prior,
    cat,
    part,
    sbuf,
    rbuf,
    tok_send,
    tok_recv,
    w_up,
    w_dn,
    w_recv,
    wx_send,
    o_up,
    o_dn,
    o_recv,
    ox_send,
    kv_send,
    kv_recv,
    pp_send,
    pp_recv,
    rs_send,
    rs_recv,
):
    G, R, TP = sizes
    s = lax.axis_index("sp")
    t = lax.axis_index("tp")
    r = s // G
    g = s % G
    head = t * G + g
    other = s + 1 - 2 * g
    chunk, feats = tok_ref.shape
    rows = G * chunk
    has_up = r + 1 < R
    has_dn = r > 0

    t_bits = []
    bit = 1
    while bit < TP:
        t_bits.append(("t", bit))
        bit *= 2
    x_dim = ("g", 1)
    members = G * TP

    def member(mask):
        gg, tt = g, t
        for kind, b in mask:
            if kind == "g":
                gg = flip(gg, b)
            else:
                tt = flip(tt, b)
        return gg, tt

    def device(mask):
        gg, tt = member(mask)
        return (r * G + gg, tt)

    barrier = pltpu.get_barrier_semaphore()
    for dim in [x_dim] + t_bits:
        pl.semaphore_signal(barrier, inc=1, device_id=device([dim]), device_id_type=MESH)

    @pl.when(has_up)
    def _():
        pl.semaphore_signal(barrier, inc=1, device_id=(s + G, t), device_id_type=MESH)

    @pl.when(has_dn)
    def _():
        pl.semaphore_signal(barrier, inc=1, device_id=(s - G, t), device_id_type=MESH)

    def pack(gg):
        a, b = gg * HEAD_DIM, (gg + 1) * HEAD_DIM
        c, d = gg * VALUE_DIM, (gg + 1) * VALUE_DIM
        wp_ref[gg, :, 0:128] = jnp.concatenate([q1_ref[:, a:b], q2_ref[:, a:b]], axis=1)
        wp_ref[gg, :, 128:256] = jnp.concatenate([k1_ref[:, a:b], k2_ref[:, a:b]], axis=1)
        wp_ref[gg, :, 256:384] = v_ref[:, c:d]
        wp_ref[gg, :, 384:512] = p_ref[:, c:d]

    for gg in range(G):
        pack(gg)

    count = 1 + len(t_bits) + jnp.where(has_up, 1, 0) + jnp.where(has_dn, 1, 0)
    pl.semaphore_wait(barrier, count)

    def rdma(src, dst, ss, rs, dev):
        return pltpu.make_async_remote_copy(
            src_ref=src, dst_ref=dst, send_sem=ss, recv_sem=rs, device_id=dev, device_id_type=MESH
        )

    def up_copy(src, buf, k, up, recv):
        return rdma(src, buf.at[k], up.at[k], recv.at[k], (s + G, t))

    def dn_copy(src, buf, k, dn, recv):
        return rdma(src, buf.at[k], dn.at[k], recv.at[k], (s - G, t))

    def send_both(src, buf, k, up, dn, recv):
        @pl.when(has_up)
        def _():
            up_copy(src, buf, k, up, recv).start()

        @pl.when(has_dn)
        def _():
            dn_copy(src, buf, k, dn, recv).start()

    def cross_copy(inp, buf, xs, recv):
        return rdma(inp.at[1 - g], buf.at[s], xs, recv.at[s], (other, t))

    def wait_slot(buf, k, up, recv):
        up_copy(buf.at[k], buf, k, up, recv).wait_recv()

    def line_step(j, buf, up, dn, recv):
        for gg in (g, 1 - g):
            @pl.when(r - 1 - j >= 0)
            def _():
                k = (r - 1 - j) * G + gg
                wait_slot(buf, k, up, recv)

                @pl.when(has_up)
                def _():
                    up_copy(buf.at[k], buf, k, up, recv).start()

            @pl.when(r + 1 + j < R)
            def _():
                k = (r + 1 + j) * G + gg
                wait_slot(buf, k, up, recv)

                @pl.when(has_dn)
                def _():
                    dn_copy(buf.at[k], buf, k, dn, recv).start()

    def drain(buf, up, dn, recv):
        @pl.when(has_up)
        def _():
            @pl.loop(0, (r + 1) * G)
            def _(k):
                up_copy(buf.at[k], buf, k, up, recv).wait_send()

        @pl.when(has_dn)
        def _():
            @pl.loop(r * G, R * G)
            def _(k):
                dn_copy(buf.at[k], buf, k, dn, recv).wait_send()

    tok_dims = t_bits[1:] + [x_dim] + t_bits[:1]
    tok_stages = []
    held = [[]]
    slot = 0
    for dim in tok_dims:
        stage = []
        for mask in held:
            gg, tt = member(mask)
            src = tok_ref if not mask else tokbuf.at[gg, tt]
            stage.append((mask, src, slot))
            slot += 1
        tok_stages.append((dim, stage))
        held = held + [mask + [dim] for mask in held]

    def tok_copy(dim, mask, src, index):
        gg, tt = member(mask)
        return rdma(src, tokbuf.at[gg, tt], tok_send.at[index], tok_recv.at[index], device([dim]))

    def tok_start(i):
        dim, stage = tok_stages[i]
        for mask, src, index in stage:
            tok_copy(dim, mask, src, index).start()

    def tok_wait(i):
        dim, stage = tok_stages[i]
        for mask, src, index in stage:
            gg, tt = member(mask + [dim])
            rdma(
                tokbuf.at[gg, tt], tokbuf.at[gg, tt], tok_send.at[index], tok_recv.at[index],
                device([dim]),
            ).wait_recv()

    send_both(wp_ref.at[g], w_all, s, w_up, w_dn, w_recv)
    cross_copy(wp_ref, w_all, wx_send, w_recv).start()
    tok_start(0)
    w_all[s] = wp_ref[g]
    tokbuf[g, t] = tok_ref[...]
    for gg in range(G):
        c, d = gg * VALUE_DIM, (gg + 1) * VALUE_DIM
        op_ref[gg, :, 0:128] = oa_ref[c:d, :].T
        op_ref[gg, :, 128:256] = ob_ref[c:d, :].T
    o_all[s] = op_ref[g]

    lane128 = lax.broadcasted_iota(jnp.int32, (chunk, 2 * HEAD_DIM), 1)
    sign = jnp.where(lane128 % HEAD_DIM < HEAD_DIM // 2, -1.0, 1.0)

    @pl.loop(0, G)
    def _(b):
        at = pl.ds(pl.multiple_of(b * chunk, chunk), chunk)
        spots = r * rows + b * chunk + lax.broadcasted_iota(jnp.int32, (chunk, 2 * HEAD_DIM), 0)
        angles = spots.astype(F32) * freq_ref[...]
        cos_ref[at, :] = jnp.cos(angles)
        sin_ref[at, :] = jnp.sin(angles) * sign

    wait_slot(w_all, other, w_up, w_recv)
    send_both(w_all.at[other], w_all, other, w_up, w_dn, w_recv)
    stage_count = len(tok_stages)
    tok_wait(0)
    tok_start(1)
    cross_copy(op_ref, o_all, ox_send, o_recv).start()
    line_step(0, w_all, w_up, w_dn, w_recv)
    for i in range(1, stage_count):
        tok_wait(i)
        if i + 1 < stage_count:
            tok_start(i + 1)
            if i < R - 1:
                line_step(i, w_all, w_up, w_dn, w_recv)
    done_steps = min(stage_count - 1, R - 1)

    def start_o():
        send_both(op_ref.at[g], o_all, s, o_up, o_dn, o_recv)
        wait_slot(o_all, other, o_up, o_recv)
        send_both(o_all.at[other], o_all, other, o_up, o_dn, o_recv)

    gain = gain_ref[...]
    width = wp_ref.shape[2]
    span = nrm.shape[2]
    tile = chunk // 2

    @pl.loop(0, G * 2)
    def _(b):
        gi = b // 2
        off = pl.multiple_of((b % 2) * tile, tile)
        dst = pl.multiple_of(b * tile, tile)
        total = jnp.zeros((tile, 1), F32)
        for i in range(TP):
            x = tokbuf[gi, i, pl.ds(off, tile), :].astype(F32)
            total = total + jnp.sum(x * x, axis=-1, keepdims=True)
        inv = lax.rsqrt(total / (TP * feats) + NORM_FLOOR)
        for i in range(TP):
            x = tokbuf[gi, i, pl.ds(off, tile), :].astype(F32)
            y = (x * inv * gain[:, i * feats : (i + 1) * feats]).astype(BF16)
            for n in range(feats // span):
                nrm[i * (feats // span) + n, pl.ds(dst, tile), :] = y[:, n * span : (n + 1) * span]

    ptile = chunk

    def project(line, first):
        @pl.loop(0, rows // ptile)
        def _(b):
            at = pl.ds(pl.multiple_of(b * ptile, ptile), ptile)
            weights = w_all[pl.ds(line * G, G)].reshape(span, width)
            y = jnp.dot(nrm[line, at, :], weights, preferred_element_type=F32)
            yacc[at, :] = y if first else yacc[at, :] + y

    def project_step(j):
        @pl.when(r - 1 - j >= 0)
        def _():
            project(r - 1 - j, False)

        @pl.when(r + 1 + j < R)
        def _():
            project(r + 1 + j, False)

    project(r, True)

    @pl.loop(0, done_steps)
    def _(j):
        project_step(j)

    if done_steps < R - 1:
        @pl.loop(done_steps, R - 1)
        def _(j):
            line_step(j, w_all, w_up, w_dn, w_recv)

            @pl.when(j == R - 2)
            def _():
                start_o()

            project_step(j)
    else:
        start_o()

    def rope(x, cosine, sine):
        lane = lax.broadcasted_iota(jnp.int32, x.shape, 1)
        near = jnp.where(
            lane % HEAD_DIM < HEAD_DIM // 2,
            pltpu.roll(x, x.shape[1] - HEAD_DIM // 2, 1),
            pltpu.roll(x, HEAD_DIM // 2, 1),
        )
        return x * cosine + near * sine

    @pl.loop(0, rows // ptile)
    def _(b):
        at = pl.ds(pl.multiple_of(b * ptile, ptile), ptile)
        y = yacc[at, :]
        cosine = cos_ref[at, :]
        sine = sin_ref[at, :]
        kv[r, at, 0:128] = rope(y[:, 128:256], cosine, sine).astype(BF16)
        kv[r, at, 128:256] = y[:, 256:384].astype(BF16)
        p = y[:, 384:512].astype(BF16)
        pool[pl.ds(pl.multiple_of(TAIL + b * ptile, TAIL), ptile), :] = p.astype(F32)
        tail[...] = p[ptile - TAIL :, :]
        q = rope(y[:, 0:128], cosine, sine).astype(BF16) * jnp.array(HEAD_DIM**-0.5, BF16)
        lane = lax.broadcasted_iota(jnp.int32, q.shape, 1)
        zero = jnp.zeros_like(q)
        q_st[0, at, :] = jnp.where(lane < HEAD_DIM, q, zero)
        q_st[1, at, :] = jnp.where(lane >= HEAD_DIM, q, zero)

    def kv_copy(k):
        return rdma(kv.at[k], kv.at[k], kv_send.at[k], kv_recv.at[k], (s + G, t))

    tail_copy = rdma(tail, prior, pp_send, pp_recv, (s + G, t))

    @pl.when(has_up)
    def _():
        kv_copy(r).start()
        tail_copy.start()

    qtile = rows // 2

    def attend(k, diagonal):
        @pl.loop(0, 4)
        def _(b):
            m_index = b // 2
            at = pl.ds(pl.multiple_of((b % 2) * qtile, qtile), qtile)
            q = q_st[m_index, at, :]
            scores = lax.dot_general(
                q, kv[k, :, 0:128], (((1,), (1,)), ((), ())), preferred_element_type=F32
            )
            if diagonal:
                qpos = (b % 2) * qtile + lax.broadcasted_iota(jnp.int32, scores.shape, 0)
                kpos = lax.broadcasted_iota(jnp.int32, scores.shape, 1)
                scores = jnp.where(kpos <= qpos, scores, MASKED)
            top = jnp.max(scores, axis=-1, keepdims=True)
            if not diagonal:
                old = m_st[m_index, at, :]
                top = jnp.maximum(old, top)
                factor = jnp.exp(old - top)
            weights = jnp.exp(scores - top)
            total = jnp.sum(weights, axis=-1, keepdims=True)
            product = jnp.dot(weights.astype(BF16), kv[k, :, 128:256], preferred_element_type=F32)
            if not diagonal:
                total = total + l_st[m_index, at, :] * factor
                product = product + acc_st[m_index, at, :] * factor
            m_st[m_index, at, :] = top
            l_st[m_index, at, :] = total
            acc_st[m_index, at, :] = product

    attend(r, True)

    @pl.loop(0, R - 1)
    def _(j):
        k = r - 1 - j

        @pl.when(j < r)
        def _():
            kv_copy(k).wait_recv()

            @pl.when(has_up)
            def _():
                kv_copy(k).start()

        @pl.when(j > 0)
        def _():
            line_step(j - 1, o_all, o_up, o_dn, o_recv)

        @pl.when(j < r)
        def _():
            attend(k, False)

    @pl.when(has_dn)
    def _():
        tail_copy.wait_recv()
        pool[0:TAIL, :] = prior[...].astype(F32)

    @pl.when(r == 0)
    def _():
        pool[0:TAIL, :] = jnp.zeros((TAIL, GROUP_DIM), F32)

    ext = pool[...]
    kind = head % 4
    window = jnp.where(kind == 0, 2, jnp.where(kind == 1, 4, jnp.where(kind == 2, 8, 16)))
    run = ext + pltpu.roll(ext, 1, 0)
    chosen = run
    for power, lag in ((1, 2), (2, 4), (3, 8)):
        run = run + pltpu.roll(run, lag, 0)
        chosen = jnp.where(kind == power, run, chosen)
    spot = r * rows + lax.broadcasted_iota(jnp.int32, (rows, GROUP_DIM), 0)
    counts = jnp.minimum(spot + 1, window).astype(F32)
    mean = chosen[TAIL:, :] / counts - ext[TAIL:, :]
    mixedg = jnp.dot(mean.astype(BF16), gw_ref[head], preferred_element_type=F32)
    cat[:, 128:256] = (mixedg * ps_ref[head]).astype(BF16)

    diff = acc_st[0] / l_st[0] - lam_ref[head] * (acc_st[1] / l_st[1])
    inv = lax.rsqrt(jnp.mean(diff * diff, axis=-1, keepdims=True) + HEAD_FLOOR)
    cat[:, 0:128] = (diff * inv * hg_ref[...] * HEAD_SCALE).astype(BF16)

    share = rows // members
    half = part.shape[2]
    o_slots = o_all.shape[0] // CHUNKS
    if R == CHUNKS:
        table = [sorted(range(R), key=lambda c: abs(c - i)) for i in range(R)]
    else:
        table = [list(range(CHUNKS))] * R

    def chunk_at(k):
        if R != CHUNKS:
            return k
        total = 0
        for i in range(R):
            total = total + jnp.where(r == i, table[i][k], 0)
        return total

    orders = ([t_bits[0], x_dim] + t_bits[1:], t_bits + [x_dim])

    def block(mask):
        gg, tt = member(mask)
        return pl.ds(pl.multiple_of((gg * TP + tt) * share, share), share)

    def combos(dims):
        found = [[]]
        for dim in dims:
            found = found + [mask + [dim] for mask in found]
        return found

    plans = []
    for h in range(CHUNKS):
        order = orders[h % 2]
        stages = []
        base = 0
        for i, dim in enumerate(order):
            masks = combos(order[i + 1 :])
            stages.append((dim, masks, base))
            base += len(masks)
        plans.append(stages)

    def rs_copy(h, dim, mask, index):
        at = block([dim] + mask)
        return rdma(
            sbuf.at[h, at, :], rbuf.at[h, index], rs_send.at[h, index], rs_recv.at[h, index],
            device([dim]),
        )

    def rs_start(h, i):
        dim, masks, base = plans[h][i]
        for n, mask in enumerate(masks):
            at = block([dim] + mask)
            sbuf[h, at, :] = part[h, at, :].astype(BF16)
        for n, mask in enumerate(masks):
            rs_copy(h, dim, mask, base + n).start()

    def rs_finish(h, i):
        dim, masks, base = plans[h][i]
        for n, mask in enumerate(masks):
            rs_copy(h, dim, mask, base + n).wait_recv()
            at = block(mask)
            part[h, at, :] = part[h, at, :] + rbuf[h, base + n].astype(F32)

    def out_product(h):
        first = chunk_at(h) * o_slots

        @pl.loop(0, 2)
        def _(b):
            at = pl.ds(pl.multiple_of(b * (rows // 2), rows // 2), rows // 2)
            columns = o_all[pl.ds(first, o_slots)].reshape(half, -1)
            part[h, at, :] = lax.dot_general(
                cat[at, :], columns, (((1,), (1,)), ((), ())), preferred_element_type=F32
            )

    levels = len(plans[0])
    mine = block([])
    if R != CHUNKS:
        line_step(R - 2, o_all, o_up, o_dn, o_recv)
    for n in range(CHUNKS + levels):
        for h in range(CHUNKS):
            i = n - 1 - h
            if 0 <= i < levels:
                rs_finish(h, i)
                if i + 1 < levels:
                    rs_start(h, i + 1)
                else:
                    at = pl.ds(pl.multiple_of(chunk_at(h) * half, half), half)
                    out_ref[:, at] = part[h, mine, :].astype(BF16)
        if n < CHUNKS:
            if n == CHUNKS - 1 and R == CHUNKS:
                line_step(R - 2, o_all, o_up, o_dn, o_recv)
            out_product(n)
            rs_start(n, 0)

    cross_copy(wp_ref, w_all, wx_send, w_recv).wait_send()
    cross_copy(op_ref, o_all, ox_send, o_recv).wait_send()
    drain(w_all, w_up, w_dn, w_recv)
    drain(o_all, o_up, o_dn, o_recv)
    for dim, stage in tok_stages:
        for mask, src, index in stage:
            tok_copy(dim, mask, src, index).wait_send()

    @pl.when(has_up)
    def _():
        tail_copy.wait_send()

        @pl.loop(0, r + 1)
        def _(k):
            kv_copy(k).wait_send()

    for h in range(CHUNKS):
        for dim, masks, base in plans[h]:
            for n, mask in enumerate(masks):
                rs_copy(h, dim, mask, base + n).wait_send()


def body(
    sp,
    tp,
    tokens,
    norm_gain,
    query_one,
    key_one,
    query_two,
    key_two,
    value_weight,
    pool_weight,
    lambda_head,
    head_gain,
    group_weight,
    pool_scale,
    out_attn,
    out_pool,
):
    G = query_one.shape[1] // HEAD_DIM
    assert G == 2 and sp % G == 0
    R = sp // G
    chunk, feats = tokens.shape
    rows = G * chunk
    depth = query_one.shape[0]
    cols = out_attn.shape[1]
    heads = lambda_head.shape[0]
    members = G * tp
    share = rows // members

    half_dim = HEAD_DIM // 2
    inverse = ROPE_BASE ** (-((np.arange(2 * HEAD_DIM) % half_dim) * 2.0 / HEAD_DIM))
    freq = jnp.asarray(inverse.astype(np.float32).reshape(1, -1))
    width = 4 * HEAD_DIM + VALUE_DIM + GROUP_DIM
    depth_out = VALUE_DIM + GROUP_DIM
    total_cols = sp * cols
    vm = pl.BlockSpec(memory_space=pltpu.VMEM)
    dma = pltpu.SemaphoreType.DMA
    return pl.pallas_call(
        functools.partial(kernel, (G, R, tp)),
        out_shape=jax.ShapeDtypeStruct((share, total_cols), BF16),
        in_specs=[vm] * 11 + [pl.BlockSpec(memory_space=pltpu.SMEM)] + [vm] * 3,
        out_specs=vm,
        scratch_shapes=[
            pltpu.VMEM((G, depth, width), BF16),
            pltpu.VMEM((G, cols, depth_out), BF16),
            pltpu.VMEM((rows, 2 * HEAD_DIM), F32),
            pltpu.VMEM((rows, 2 * HEAD_DIM), F32),
            pltpu.VMEM((rows, width), F32),
            pltpu.VMEM((G, tp, chunk, feats), BF16),
            pltpu.VMEM((R, rows, G * depth), BF16),
            pltpu.VMEM((sp, depth, width), BF16),
            pltpu.VMEM((sp, cols, depth_out), BF16),
            pltpu.VMEM((R, rows, 256), BF16),
            pltpu.VMEM((2, rows, 128), BF16),
            pltpu.VMEM((2, rows, 1), F32),
            pltpu.VMEM((2, rows, 1), F32),
            pltpu.VMEM((2, rows, VALUE_DIM), F32),
            pltpu.VMEM((TAIL + rows, GROUP_DIM), F32),
            pltpu.VMEM((TAIL, GROUP_DIM), BF16),
            pltpu.VMEM((TAIL, GROUP_DIM), BF16),
            pltpu.VMEM((rows, depth_out), BF16),
            pltpu.VMEM((CHUNKS, rows, total_cols // CHUNKS), F32),
            pltpu.VMEM((CHUNKS, rows, total_cols // CHUNKS), BF16),
            pltpu.VMEM((CHUNKS, members - 1, share, total_cols // CHUNKS), BF16),
            dma((members - 1,)),
            dma((members - 1,)),
            dma((sp,)),
            dma((sp,)),
            dma((sp,)),
            dma,
            dma((sp,)),
            dma((sp,)),
            dma((sp,)),
            dma,
            dma((R,)),
            dma((R,)),
            dma,
            dma,
            dma((CHUNKS, members - 1)),
            dma((CHUNKS, members - 1)),
        ],
        compiler_params=pltpu.CompilerParams(
            collective_id=0, has_side_effects=True, vmem_limit_bytes=58 * 1024 * 1024
        ),
    )(
        tokens,
        norm_gain.reshape(1, -1),
        query_one,
        key_one,
        query_two,
        key_two,
        value_weight,
        pool_weight,
        out_attn,
        out_pool,
        freq,
        lambda_head,
        head_gain.reshape(1, -1),
        group_weight,
        pool_scale.reshape(heads, 1, GROUP_DIM),
    )


def solution(mesh):
    in_specs = (
        P("sp", "tp"),
        P(),
        P("sp", "tp"),
        P("sp", "tp"),
        P("sp", "tp"),
        P("sp", "tp"),
        P("sp", "tp"),
        P("sp", "tp"),
        P(),
        P(),
        P(),
        P(),
        P("tp", "sp"),
        P("tp", "sp"),
    )
    return jax.shard_map(
        functools.partial(body, mesh.shape["sp"], mesh.shape["tp"]),
        mesh=mesh,
        in_specs=in_specs,
        out_specs=P(("sp", "tp"), None),
        check_vma=False,
    )
```

```python
import functools

import jax
import jax.numpy as jnp
import numpy as np
from jax import lax
from jax.experimental import pallas as pl
from jax.experimental.pallas import tpu as pltpu
from jax.sharding import PartitionSpec as P

HEAD_DIM = 64
VALUE_DIM = 128
GROUP_DIM = 128
ROPE_BASE = 500000.0
HEAD_SCALE = 0.8
NORM_FLOOR = 1e-06
HEAD_FLOOR = 0.001
MASKED = -1e30
TAIL = 16
CHUNKS = 8
PARTS = 2
MESH = pl.DeviceIdType.MESH
BF16 = jnp.bfloat16
F32 = jnp.float32


def flip(index, bit):
    return index + bit * (1 - 2 * ((index // bit) % 2))


def kernel(
    sizes,
    tok_ref,
    gain_ref,
    q1_ref,
    k1_ref,
    q2_ref,
    k2_ref,
    v_ref,
    p_ref,
    oa_ref,
    ob_ref,
    freq_ref,
    lam_ref,
    hg_ref,
    gw_ref,
    ps_ref,
    out_ref,
    wp_ref,
    op_ref,
    cos_ref,
    sin_ref,
    yacc,
    tokbuf,
    nrm,
    w_all,
    o_all,
    kv,
    q_st,
    m_st,
    l_st,
    acc_st,
    pool,
    tail,
    prior,
    cat,
    part,
    sbuf,
    rbuf,
    tok_send,
    tok_recv,
    w_up,
    w_dn,
    w_recv,
    wx_send,
    o_up,
    o_dn,
    o_recv,
    ox_send,
    kv_send,
    kv_recv,
    pp_send,
    pp_recv,
    rs_send,
    rs_recv,
):
    G, R, TP = sizes
    s = lax.axis_index("sp")
    t = lax.axis_index("tp")
    r = s // G
    g = s % G
    head = t * G + g
    other = s + 1 - 2 * g
    chunk, feats = tok_ref.shape
    rows = G * chunk
    has_up = r + 1 < R
    has_dn = r > 0

    t_bits = []
    bit = 1
    while bit < TP:
        t_bits.append(("t", bit))
        bit *= 2
    x_dim = ("g", 1)
    members = G * TP

    def member(mask):
        gg, tt = g, t
        for kind, b in mask:
            if kind == "g":
                gg = flip(gg, b)
            else:
                tt = flip(tt, b)
        return gg, tt

    def device(mask):
        gg, tt = member(mask)
        return (r * G + gg, tt)

    barrier = pltpu.get_barrier_semaphore()
    for dim in [x_dim] + t_bits:
        pl.semaphore_signal(barrier, inc=1, device_id=device([dim]), device_id_type=MESH)

    @pl.when(has_up)
    def _():
        pl.semaphore_signal(barrier, inc=1, device_id=(s + G, t), device_id_type=MESH)

    @pl.when(has_dn)
    def _():
        pl.semaphore_signal(barrier, inc=1, device_id=(s - G, t), device_id_type=MESH)

    def pack(gg):
        a, b = gg * HEAD_DIM, (gg + 1) * HEAD_DIM
        c, d = gg * VALUE_DIM, (gg + 1) * VALUE_DIM
        wp_ref[gg, :, 0:128] = jnp.concatenate([q1_ref[:, a:b], q2_ref[:, a:b]], axis=1)
        wp_ref[gg, :, 128:256] = jnp.concatenate([k1_ref[:, a:b], k2_ref[:, a:b]], axis=1)
        wp_ref[gg, :, 256:384] = v_ref[:, c:d]
        wp_ref[gg, :, 384:512] = p_ref[:, c:d]

    for gg in range(G):
        pack(gg)

    count = 1 + len(t_bits) + jnp.where(has_up, 1, 0) + jnp.where(has_dn, 1, 0)
    pl.semaphore_wait(barrier, count)

    def rdma(src, dst, ss, rs, dev):
        return pltpu.make_async_remote_copy(
            src_ref=src, dst_ref=dst, send_sem=ss, recv_sem=rs, device_id=dev, device_id_type=MESH
        )

    def up_copy(src, buf, k, up, recv):
        return rdma(src, buf.at[k], up.at[k], recv.at[k], (s + G, t))

    def dn_copy(src, buf, k, dn, recv):
        return rdma(src, buf.at[k], dn.at[k], recv.at[k], (s - G, t))

    def send_both(src, buf, k, up, dn, recv):
        @pl.when(has_up)
        def _():
            up_copy(src, buf, k, up, recv).start()

        @pl.when(has_dn)
        def _():
            dn_copy(src, buf, k, dn, recv).start()

    def cross_copy(inp, buf, xs, recv):
        return rdma(inp.at[1 - g], buf.at[s], xs, recv.at[s], (other, t))

    def wait_slot(buf, k, up, recv):
        up_copy(buf.at[k], buf, k, up, recv).wait_recv()

    def line_step(j, buf, up, dn, recv):
        for gg in (g, 1 - g):
            @pl.when(r - 1 - j >= 0)
            def _():
                k = (r - 1 - j) * G + gg
                wait_slot(buf, k, up, recv)

                @pl.when(has_up)
                def _():
                    up_copy(buf.at[k], buf, k, up, recv).start()

            @pl.when(r + 1 + j < R)
            def _():
                k = (r + 1 + j) * G + gg
                wait_slot(buf, k, up, recv)

                @pl.when(has_dn)
                def _():
                    dn_copy(buf.at[k], buf, k, dn, recv).start()

    def drain(buf, up, dn, recv):
        @pl.when(has_up)
        def _():
            @pl.loop(0, (r + 1) * G)
            def _(k):
                up_copy(buf.at[k], buf, k, up, recv).wait_send()

        @pl.when(has_dn)
        def _():
            @pl.loop(r * G, R * G)
            def _(k):
                dn_copy(buf.at[k], buf, k, dn, recv).wait_send()

    tok_dims = t_bits[1:] + [x_dim] + t_bits[:1]
    tok_stages = []
    held = [[]]
    slot = 0
    for dim in tok_dims:
        stage = []
        for mask in held:
            gg, tt = member(mask)
            src = tok_ref if not mask else tokbuf.at[gg, tt]
            stage.append((mask, src, slot))
            slot += 1
        tok_stages.append((dim, stage))
        held = held + [mask + [dim] for mask in held]

    def tok_copy(dim, mask, src, index):
        gg, tt = member(mask)
        return rdma(src, tokbuf.at[gg, tt], tok_send.at[index], tok_recv.at[index], device([dim]))

    def tok_start(i):
        dim, stage = tok_stages[i]
        for mask, src, index in stage:
            tok_copy(dim, mask, src, index).start()

    def tok_wait(i):
        dim, stage = tok_stages[i]
        for mask, src, index in stage:
            gg, tt = member(mask + [dim])
            rdma(
                tokbuf.at[gg, tt], tokbuf.at[gg, tt], tok_send.at[index], tok_recv.at[index],
                device([dim]),
            ).wait_recv()

    send_both(wp_ref.at[g], w_all, s, w_up, w_dn, w_recv)
    cross_copy(wp_ref, w_all, wx_send, w_recv).start()
    tok_start(0)
    w_all[s] = wp_ref[g]
    tokbuf[g, t] = tok_ref[...]
    for gg in range(G):
        c, d = gg * VALUE_DIM, (gg + 1) * VALUE_DIM
        op_ref[gg, :, 0:128] = oa_ref[c:d, :].T
        op_ref[gg, :, 128:256] = ob_ref[c:d, :].T
    o_all[s] = op_ref[g]

    lane128 = lax.broadcasted_iota(jnp.int32, (chunk, 2 * HEAD_DIM), 1)
    sign = jnp.where(lane128 % HEAD_DIM < HEAD_DIM // 2, -1.0, 1.0)

    @pl.loop(0, G)
    def _(b):
        at = pl.ds(pl.multiple_of(b * chunk, chunk), chunk)
        spots = r * rows + b * chunk + lax.broadcasted_iota(jnp.int32, (chunk, 2 * HEAD_DIM), 0)
        angles = spots.astype(F32) * freq_ref[...]
        cos_ref[at, :] = jnp.cos(angles)
        sin_ref[at, :] = jnp.sin(angles) * sign

    wait_slot(w_all, other, w_up, w_recv)
    send_both(w_all.at[other], w_all, other, w_up, w_dn, w_recv)
    stage_count = len(tok_stages)
    tok_wait(0)
    tok_start(1)
    cross_copy(op_ref, o_all, ox_send, o_recv).start()
    line_step(0, w_all, w_up, w_dn, w_recv)
    for i in range(1, stage_count):
        tok_wait(i)
        if i + 1 < stage_count:
            tok_start(i + 1)
            if i < R - 1:
                line_step(i, w_all, w_up, w_dn, w_recv)
    done_steps = min(stage_count - 1, R - 1)

    def start_o():
        send_both(op_ref.at[g], o_all, s, o_up, o_dn, o_recv)
        wait_slot(o_all, other, o_up, o_recv)
        send_both(o_all.at[other], o_all, other, o_up, o_dn, o_recv)

    gain = gain_ref[...]
    width = wp_ref.shape[2]
    span = nrm.shape[2]
    tile = chunk // 2

    @pl.loop(0, G * 2)
    def _(b):
        gi = b // 2
        off = pl.multiple_of((b % 2) * tile, tile)
        dst = pl.multiple_of(b * tile, tile)
        total = jnp.zeros((tile, 1), F32)
        for i in range(TP):
            x = tokbuf[gi, i, pl.ds(off, tile), :].astype(F32)
            total = total + jnp.sum(x * x, axis=-1, keepdims=True)
        inv = lax.rsqrt(total / (TP * feats) + NORM_FLOOR)
        for i in range(TP):
            x = tokbuf[gi, i, pl.ds(off, tile), :].astype(F32)
            y = (x * inv * gain[:, i * feats : (i + 1) * feats]).astype(BF16)
            for n in range(feats // span):
                nrm[i * (feats // span) + n, pl.ds(dst, tile), :] = y[:, n * span : (n + 1) * span]

    ptile = chunk

    def project(line, first):
        @pl.loop(0, rows // ptile)
        def _(b):
            at = pl.ds(pl.multiple_of(b * ptile, ptile), ptile)
            weights = w_all[pl.ds(line * G, G)].reshape(span, width)
            y = jnp.dot(nrm[line, at, :], weights, preferred_element_type=F32)
            yacc[at, :] = y if first else yacc[at, :] + y

    def project_step(j):
        @pl.when(r - 1 - j >= 0)
        def _():
            project(r - 1 - j, False)

        @pl.when(r + 1 + j < R)
        def _():
            project(r + 1 + j, False)

    project(r, True)

    @pl.loop(0, done_steps)
    def _(j):
        project_step(j)

    if done_steps < R - 1:
        @pl.loop(done_steps, R - 1)
        def _(j):
            line_step(j, w_all, w_up, w_dn, w_recv)

            @pl.when(j == R - 2)
            def _():
                start_o()

            project_step(j)
    else:
        start_o()

    def rope(x, cosine, sine):
        lane = lax.broadcasted_iota(jnp.int32, x.shape, 1)
        near = jnp.where(
            lane % HEAD_DIM < HEAD_DIM // 2,
            pltpu.roll(x, x.shape[1] - HEAD_DIM // 2, 1),
            pltpu.roll(x, HEAD_DIM // 2, 1),
        )
        return x * cosine + near * sine

    @pl.loop(0, rows // ptile)
    def _(b):
        at = pl.ds(pl.multiple_of(b * ptile, ptile), ptile)
        y = yacc[at, :]
        cosine = cos_ref[at, :]
        sine = sin_ref[at, :]
        kv[r, at, 0:128] = rope(y[:, 128:256], cosine, sine).astype(BF16)
        kv[r, at, 128:256] = y[:, 256:384].astype(BF16)
        p = y[:, 384:512].astype(BF16)
        pool[pl.ds(pl.multiple_of(TAIL + b * ptile, TAIL), ptile), :] = p.astype(F32)
        tail[...] = p[ptile - TAIL :, :]
        q = rope(y[:, 0:128], cosine, sine).astype(BF16) * jnp.array(HEAD_DIM**-0.5, BF16)
        lane = lax.broadcasted_iota(jnp.int32, q.shape, 1)
        zero = jnp.zeros_like(q)
        q_st[0, at, :] = jnp.where(lane < HEAD_DIM, q, zero)
        q_st[1, at, :] = jnp.where(lane >= HEAD_DIM, q, zero)

    def kv_copy(k):
        return rdma(kv.at[k], kv.at[k], kv_send.at[k], kv_recv.at[k], (s + G, t))

    tail_copy = rdma(tail, prior, pp_send, pp_recv, (s + G, t))

    @pl.when(has_up)
    def _():
        kv_copy(r).start()
        tail_copy.start()

    qtile = rows // 2

    def attend(k, diagonal):
        @pl.loop(0, 4)
        def _(b):
            m_index = b // 2
            at = pl.ds(pl.multiple_of((b % 2) * qtile, qtile), qtile)
            q = q_st[m_index, at, :]
            scores = lax.dot_general(
                q, kv[k, :, 0:128], (((1,), (1,)), ((), ())), preferred_element_type=F32
            )
            if diagonal:
                qpos = (b % 2) * qtile + lax.broadcasted_iota(jnp.int32, scores.shape, 0)
                kpos = lax.broadcasted_iota(jnp.int32, scores.shape, 1)
                scores = jnp.where(kpos <= qpos, scores, MASKED)
            top = jnp.max(scores, axis=-1, keepdims=True)
            if not diagonal:
                old = m_st[m_index, at, :]
                top = jnp.maximum(old, top)
                factor = jnp.exp(old - top)
            weights = jnp.exp(scores - top)
            total = jnp.sum(weights, axis=-1, keepdims=True)
            product = jnp.dot(weights.astype(BF16), kv[k, :, 128:256], preferred_element_type=F32)
            if not diagonal:
                total = total + l_st[m_index, at, :] * factor
                product = product + acc_st[m_index, at, :] * factor
            m_st[m_index, at, :] = top
            l_st[m_index, at, :] = total
            acc_st[m_index, at, :] = product

    attend(r, True)

    @pl.loop(0, R - 1)
    def _(j):
        k = r - 1 - j

        @pl.when(j < r)
        def _():
            kv_copy(k).wait_recv()

            @pl.when(has_up)
            def _():
                kv_copy(k).start()

        @pl.when(j > 0)
        def _():
            line_step(j - 1, o_all, o_up, o_dn, o_recv)

        @pl.when(j < r)
        def _():
            attend(k, False)

    @pl.when(has_dn)
    def _():
        tail_copy.wait_recv()
        pool[0:TAIL, :] = prior[...].astype(F32)

    @pl.when(r == 0)
    def _():
        pool[0:TAIL, :] = jnp.zeros((TAIL, GROUP_DIM), F32)

    ext = pool[...]
    kind = head % 4
    window = jnp.where(kind == 0, 2, jnp.where(kind == 1, 4, jnp.where(kind == 2, 8, 16)))
    run = ext + pltpu.roll(ext, 1, 0)
    chosen = run
    for power, lag in ((1, 2), (2, 4), (3, 8)):
        run = run + pltpu.roll(run, lag, 0)
        chosen = jnp.where(kind == power, run, chosen)
    spot = r * rows + lax.broadcasted_iota(jnp.int32, (rows, GROUP_DIM), 0)
    counts = jnp.minimum(spot + 1, window).astype(F32)
    mean = chosen[TAIL:, :] / counts - ext[TAIL:, :]
    mixedg = jnp.dot(mean.astype(BF16), gw_ref[head], preferred_element_type=F32)
    cat[:, 128:256] = (mixedg * ps_ref[head]).astype(BF16)

    diff = acc_st[0] / l_st[0] - lam_ref[head] * (acc_st[1] / l_st[1])
    inv = lax.rsqrt(jnp.mean(diff * diff, axis=-1, keepdims=True) + HEAD_FLOOR)
    cat[:, 0:128] = (diff * inv * hg_ref[...] * HEAD_SCALE).astype(BF16)

    share = rows // members
    half = part.shape[2]
    o_slots = o_all.shape[0] // CHUNKS
    by_line = R * PARTS == CHUNKS
    table = [sorted(range(R), key=lambda c: abs(c - i)) for i in range(R)]

    def chunk_at(k):
        if not by_line:
            return k
        total = 0
        for i in range(R):
            total = total + jnp.where(r == i, table[i][k // PARTS], 0)
        return total * PARTS + k % PARTS

    orders = ([t_bits[0], x_dim] + t_bits[1:], t_bits + [x_dim])

    def block(mask):
        gg, tt = member(mask)
        return pl.ds(pl.multiple_of((gg * TP + tt) * share, share), share)

    def combos(dims):
        found = [[]]
        for dim in dims:
            found = found + [mask + [dim] for mask in found]
        return found

    plans = []
    for h in range(CHUNKS):
        order = orders[h % 2]
        stages = []
        base = 0
        for i, dim in enumerate(order):
            masks = combos(order[i + 1 :])
            stages.append((dim, masks, base))
            base += len(masks)
        plans.append(stages)

    def rs_copy(h, dim, mask, index):
        at = block([dim] + mask)
        return rdma(
            sbuf.at[h, at, :], rbuf.at[h, index], rs_send.at[h, index], rs_recv.at[h, index],
            device([dim]),
        )

    def rs_start(h, i):
        dim, masks, base = plans[h][i]
        for n, mask in enumerate(masks):
            at = block([dim] + mask)
            sbuf[h, at, :] = part[h, at, :].astype(BF16)
        for n, mask in enumerate(masks):
            rs_copy(h, dim, mask, base + n).start()

    def rs_finish(h, i):
        dim, masks, base = plans[h][i]
        for n, mask in enumerate(masks):
            rs_copy(h, dim, mask, base + n).wait_recv()
            at = block(mask)
            part[h, at, :] = part[h, at, :] + rbuf[h, base + n].astype(F32)

    def out_product(h):
        first = chunk_at(h) * o_slots

        @pl.loop(0, 2)
        def _(b):
            at = pl.ds(pl.multiple_of(b * (rows // 2), rows // 2), rows // 2)
            columns = o_all[pl.ds(first, o_slots)].reshape(half, -1)
            part[h, at, :] = lax.dot_general(
                cat[at, :], columns, (((1,), (1,)), ((), ())), preferred_element_type=F32
            )

    levels = len(plans[0])
    mine = block([])
    last = lambda: line_step(R - 2, o_all, o_up, o_dn, o_recv)
    if by_line:
        batches = [range(CHUNKS - PARTS), range(CHUNKS - PARTS, CHUNKS)]
    else:
        batches = [range(CHUNKS)]
    for n, batch in enumerate(batches):
        if n == len(batches) - 1:
            last()
        for h in batch:
            out_product(h)
            rs_start(h, 0)
        for i in range(levels):
            for h in batch:
                rs_finish(h, i)
                if i + 1 < levels:
                    rs_start(h, i + 1)
                else:
                    at = pl.ds(pl.multiple_of(chunk_at(h) * half, half), half)
                    out_ref[:, at] = part[h, mine, :].astype(BF16)

    cross_copy(wp_ref, w_all, wx_send, w_recv).wait_send()
    cross_copy(op_ref, o_all, ox_send, o_recv).wait_send()
    drain(w_all, w_up, w_dn, w_recv)
    drain(o_all, o_up, o_dn, o_recv)
    for dim, stage in tok_stages:
        for mask, src, index in stage:
            tok_copy(dim, mask, src, index).wait_send()

    @pl.when(has_up)
    def _():
        tail_copy.wait_send()

        @pl.loop(0, r + 1)
        def _(k):
            kv_copy(k).wait_send()

    for h in range(CHUNKS):
        for dim, masks, base in plans[h]:
            for n, mask in enumerate(masks):
                rs_copy(h, dim, mask, base + n).wait_send()


def body(
    sp,
    tp,
    tokens,
    norm_gain,
    query_one,
    key_one,
    query_two,
    key_two,
    value_weight,
    pool_weight,
    lambda_head,
    head_gain,
    group_weight,
    pool_scale,
    out_attn,
    out_pool,
):
    G = query_one.shape[1] // HEAD_DIM
    assert G == 2 and sp % G == 0
    R = sp // G
    chunk, feats = tokens.shape
    rows = G * chunk
    depth = query_one.shape[0]
    cols = out_attn.shape[1]
    heads = lambda_head.shape[0]
    members = G * tp
    share = rows // members

    half_dim = HEAD_DIM // 2
    inverse = ROPE_BASE ** (-((np.arange(2 * HEAD_DIM) % half_dim) * 2.0 / HEAD_DIM))
    freq = jnp.asarray(inverse.astype(np.float32).reshape(1, -1))
    width = 4 * HEAD_DIM + VALUE_DIM + GROUP_DIM
    depth_out = VALUE_DIM + GROUP_DIM
    total_cols = sp * cols
    vm = pl.BlockSpec(memory_space=pltpu.VMEM)
    dma = pltpu.SemaphoreType.DMA
    return pl.pallas_call(
        functools.partial(kernel, (G, R, tp)),
        out_shape=jax.ShapeDtypeStruct((share, total_cols), BF16),
        in_specs=[vm] * 11 + [pl.BlockSpec(memory_space=pltpu.SMEM)] + [vm] * 3,
        out_specs=vm,
        scratch_shapes=[
            pltpu.VMEM((G, depth, width), BF16),
            pltpu.VMEM((G, cols, depth_out), BF16),
            pltpu.VMEM((rows, 2 * HEAD_DIM), F32),
            pltpu.VMEM((rows, 2 * HEAD_DIM), F32),
            pltpu.VMEM((rows, width), F32),
            pltpu.VMEM((G, tp, chunk, feats), BF16),
            pltpu.VMEM((R, rows, G * depth), BF16),
            pltpu.VMEM((sp, depth, width), BF16),
            pltpu.VMEM((sp, cols, depth_out), BF16),
            pltpu.VMEM((R, rows, 256), BF16),
            pltpu.VMEM((2, rows, 128), BF16),
            pltpu.VMEM((2, rows, 1), F32),
            pltpu.VMEM((2, rows, 1), F32),
            pltpu.VMEM((2, rows, VALUE_DIM), F32),
            pltpu.VMEM((TAIL + rows, GROUP_DIM), F32),
            pltpu.VMEM((TAIL, GROUP_DIM), BF16),
            pltpu.VMEM((TAIL, GROUP_DIM), BF16),
            pltpu.VMEM((rows, depth_out), BF16),
            pltpu.VMEM((CHUNKS, rows, total_cols // CHUNKS), F32),
            pltpu.VMEM((CHUNKS, rows, total_cols // CHUNKS), BF16),
            pltpu.VMEM((CHUNKS, members - 1, share, total_cols // CHUNKS), BF16),
            dma((members - 1,)),
            dma((members - 1,)),
            dma((sp,)),
            dma((sp,)),
            dma((sp,)),
            dma,
            dma((sp,)),
            dma((sp,)),
            dma((sp,)),
            dma,
            dma((R,)),
            dma((R,)),
            dma,
            dma,
            dma((CHUNKS, members - 1)),
            dma((CHUNKS, members - 1)),
        ],
        compiler_params=pltpu.CompilerParams(
            collective_id=0, has_side_effects=True, vmem_limit_bytes=58 * 1024 * 1024
        ),
    )(
        tokens,
        norm_gain.reshape(1, -1),
        query_one,
        key_one,
        query_two,
        key_two,
        value_weight,
        pool_weight,
        out_attn,
        out_pool,
        freq,
        lambda_head,
        head_gain.reshape(1, -1),
        group_weight,
        pool_scale.reshape(heads, 1, GROUP_DIM),
    )


def solution(mesh):
    in_specs = (
        P("sp", "tp"),
        P(),
        P("sp", "tp"),
        P("sp", "tp"),
        P("sp", "tp"),
        P("sp", "tp"),
        P("sp", "tp"),
        P("sp", "tp"),
        P(),
        P(),
        P(),
        P(),
        P("tp", "sp"),
        P("tp", "sp"),
    )
    return jax.shard_map(
        functools.partial(body, mesh.shape["sp"], mesh.shape["tp"]),
        mesh=mesh,
        in_specs=in_specs,
        out_specs=P(("sp", "tp"), None),
        check_vma=False,
    )
```

```python
import functools

import jax
import jax.numpy as jnp
import numpy as np
from jax import lax
from jax.experimental import pallas as pl
from jax.experimental.pallas import tpu as pltpu
from jax.sharding import PartitionSpec as P

HEAD_DIM = 64
VALUE_DIM = 128
GROUP_DIM = 128
ROPE_BASE = 500000.0
HEAD_SCALE = 0.8
NORM_FLOOR = 1e-06
HEAD_FLOOR = 0.001
MASKED = -1e30
TAIL = 16
CHUNKS = 8
PARTS = 2
MESH = pl.DeviceIdType.MESH
BF16 = jnp.bfloat16
F32 = jnp.float32


def flip(index, bit):
    return index + bit * (1 - 2 * ((index // bit) % 2))


def kernel(
    sizes,
    tok_ref,
    gain_ref,
    q1_ref,
    k1_ref,
    q2_ref,
    k2_ref,
    v_ref,
    p_ref,
    oa_ref,
    ob_ref,
    freq_ref,
    lam_ref,
    hg_ref,
    gw_ref,
    ps_ref,
    out_ref,
    wp_ref,
    op_ref,
    cos_ref,
    sin_ref,
    yacc,
    tokbuf,
    nrm,
    w_all,
    o_all,
    kv,
    q_st,
    m_st,
    l_st,
    acc_st,
    pool,
    tail,
    prior,
    cat,
    part,
    sbuf,
    rbuf,
    tok_send,
    tok_recv,
    w_up,
    w_dn,
    w_recv,
    wx_send,
    o_up,
    o_dn,
    o_recv,
    ox_send,
    kv_send,
    kv_recv,
    pp_send,
    pp_recv,
    rs_send,
    rs_recv,
):
    G, R, TP = sizes
    s = lax.axis_index("sp")
    t = lax.axis_index("tp")
    r = s // G
    g = s % G
    head = t * G + g
    other = s + 1 - 2 * g
    chunk, feats = tok_ref.shape
    rows = G * chunk
    has_up = r + 1 < R
    has_dn = r > 0

    t_bits = []
    bit = 1
    while bit < TP:
        t_bits.append(("t", bit))
        bit *= 2
    x_dim = ("g", 1)
    members = G * TP

    def member(mask):
        gg, tt = g, t
        for kind, b in mask:
            if kind == "g":
                gg = flip(gg, b)
            else:
                tt = flip(tt, b)
        return gg, tt

    def device(mask):
        gg, tt = member(mask)
        return (r * G + gg, tt)

    barrier = pltpu.get_barrier_semaphore()
    for dim in [x_dim] + t_bits:
        pl.semaphore_signal(barrier, inc=1, device_id=device([dim]), device_id_type=MESH)

    @pl.when(has_up)
    def _():
        pl.semaphore_signal(barrier, inc=1, device_id=(s + G, t), device_id_type=MESH)

    @pl.when(has_dn)
    def _():
        pl.semaphore_signal(barrier, inc=1, device_id=(s - G, t), device_id_type=MESH)

    def pack(gg):
        a, b = gg * HEAD_DIM, (gg + 1) * HEAD_DIM
        c, d = gg * VALUE_DIM, (gg + 1) * VALUE_DIM
        wp_ref[gg, :, 0:128] = jnp.concatenate([q1_ref[:, a:b], q2_ref[:, a:b]], axis=1)
        wp_ref[gg, :, 128:256] = jnp.concatenate([k1_ref[:, a:b], k2_ref[:, a:b]], axis=1)
        wp_ref[gg, :, 256:384] = v_ref[:, c:d]
        wp_ref[gg, :, 384:512] = p_ref[:, c:d]

    for gg in range(G):
        pack(gg)

    count = 1 + len(t_bits) + jnp.where(has_up, 1, 0) + jnp.where(has_dn, 1, 0)
    pl.semaphore_wait(barrier, count)

    def rdma(src, dst, ss, rs, dev):
        return pltpu.make_async_remote_copy(
            src_ref=src, dst_ref=dst, send_sem=ss, recv_sem=rs, device_id=dev, device_id_type=MESH
        )

    def up_copy(src, buf, k, up, recv):
        return rdma(src, buf.at[k], up.at[k], recv.at[k], (s + G, t))

    def dn_copy(src, buf, k, dn, recv):
        return rdma(src, buf.at[k], dn.at[k], recv.at[k], (s - G, t))

    def send_both(src, buf, k, up, dn, recv):
        @pl.when(has_up)
        def _():
            up_copy(src, buf, k, up, recv).start()

        @pl.when(has_dn)
        def _():
            dn_copy(src, buf, k, dn, recv).start()

    def cross_copy(inp, buf, xs, recv):
        return rdma(inp.at[1 - g], buf.at[s], xs, recv.at[s], (other, t))

    def wait_slot(buf, k, up, recv):
        up_copy(buf.at[k], buf, k, up, recv).wait_recv()

    def line_step(j, buf, up, dn, recv):
        for gg in (g, 1 - g):
            @pl.when(r - 1 - j >= 0)
            def _():
                k = (r - 1 - j) * G + gg
                wait_slot(buf, k, up, recv)

                @pl.when(has_up)
                def _():
                    up_copy(buf.at[k], buf, k, up, recv).start()

            @pl.when(r + 1 + j < R)
            def _():
                k = (r + 1 + j) * G + gg
                wait_slot(buf, k, up, recv)

                @pl.when(has_dn)
                def _():
                    dn_copy(buf.at[k], buf, k, dn, recv).start()

    def drain(buf, up, dn, recv):
        @pl.when(has_up)
        def _():
            @pl.loop(0, (r + 1) * G)
            def _(k):
                up_copy(buf.at[k], buf, k, up, recv).wait_send()

        @pl.when(has_dn)
        def _():
            @pl.loop(r * G, R * G)
            def _(k):
                dn_copy(buf.at[k], buf, k, dn, recv).wait_send()

    tok_dims = t_bits[1:] + [x_dim] + t_bits[:1]
    tok_stages = []
    held = [[]]
    slot = 0
    for dim in tok_dims:
        stage = []
        for mask in held:
            gg, tt = member(mask)
            src = tok_ref if not mask else tokbuf.at[gg, tt]
            stage.append((mask, src, slot))
            slot += 1
        tok_stages.append((dim, stage))
        held = held + [mask + [dim] for mask in held]

    def tok_copy(dim, mask, src, index):
        gg, tt = member(mask)
        return rdma(src, tokbuf.at[gg, tt], tok_send.at[index], tok_recv.at[index], device([dim]))

    def tok_start(i):
        dim, stage = tok_stages[i]
        for mask, src, index in stage:
            tok_copy(dim, mask, src, index).start()

    def tok_wait(i):
        dim, stage = tok_stages[i]
        for mask, src, index in stage:
            gg, tt = member(mask + [dim])
            rdma(
                tokbuf.at[gg, tt], tokbuf.at[gg, tt], tok_send.at[index], tok_recv.at[index],
                device([dim]),
            ).wait_recv()

    send_both(wp_ref.at[g], w_all, s, w_up, w_dn, w_recv)
    cross_copy(wp_ref, w_all, wx_send, w_recv).start()
    tok_start(0)
    w_all[s] = wp_ref[g]
    tokbuf[g, t] = tok_ref[...]
    for gg in range(G):
        c, d = gg * VALUE_DIM, (gg + 1) * VALUE_DIM
        op_ref[gg, :, 0:128] = oa_ref[c:d, :].T
        op_ref[gg, :, 128:256] = ob_ref[c:d, :].T
    o_all[s] = op_ref[g]

    lane128 = lax.broadcasted_iota(jnp.int32, (chunk, 2 * HEAD_DIM), 1)
    sign = jnp.where(lane128 % HEAD_DIM < HEAD_DIM // 2, -1.0, 1.0)

    @pl.loop(0, G)
    def _(b):
        at = pl.ds(pl.multiple_of(b * chunk, chunk), chunk)
        spots = r * rows + b * chunk + lax.broadcasted_iota(jnp.int32, (chunk, 2 * HEAD_DIM), 0)
        angles = spots.astype(F32) * freq_ref[...]
        cos_ref[at, :] = jnp.cos(angles)
        sin_ref[at, :] = jnp.sin(angles) * sign

    wait_slot(w_all, other, w_up, w_recv)
    send_both(w_all.at[other], w_all, other, w_up, w_dn, w_recv)
    stage_count = len(tok_stages)
    tok_wait(0)
    tok_start(1)
    cross_copy(op_ref, o_all, ox_send, o_recv).start()
    line_step(0, w_all, w_up, w_dn, w_recv)
    for i in range(1, stage_count):
        tok_wait(i)
        if i + 1 < stage_count:
            tok_start(i + 1)
            if i < R - 1:
                line_step(i, w_all, w_up, w_dn, w_recv)
    done_steps = min(stage_count - 1, R - 1)

    def start_o():
        send_both(op_ref.at[g], o_all, s, o_up, o_dn, o_recv)
        wait_slot(o_all, other, o_up, o_recv)
        send_both(o_all.at[other], o_all, other, o_up, o_dn, o_recv)

    gain = gain_ref[...]
    width = wp_ref.shape[2]
    span = nrm.shape[2]
    tile = chunk // 2

    @pl.loop(0, G * 2)
    def _(b):
        gi = b // 2
        off = pl.multiple_of((b % 2) * tile, tile)
        dst = pl.multiple_of(b * tile, tile)
        total = jnp.zeros((tile, 1), F32)
        for i in range(TP):
            x = tokbuf[gi, i, pl.ds(off, tile), :].astype(F32)
            total = total + jnp.sum(x * x, axis=-1, keepdims=True)
        inv = lax.rsqrt(total / (TP * feats) + NORM_FLOOR)
        for i in range(TP):
            x = tokbuf[gi, i, pl.ds(off, tile), :].astype(F32)
            y = (x * inv * gain[:, i * feats : (i + 1) * feats]).astype(BF16)
            for n in range(feats // span):
                nrm[i * (feats // span) + n, pl.ds(dst, tile), :] = y[:, n * span : (n + 1) * span]

    ptile = chunk

    def project(line, first):
        @pl.loop(0, rows // ptile)
        def _(b):
            at = pl.ds(pl.multiple_of(b * ptile, ptile), ptile)
            weights = w_all[pl.ds(line * G, G)].reshape(span, width)
            y = jnp.dot(nrm[line, at, :], weights, preferred_element_type=F32)
            yacc[at, :] = y if first else yacc[at, :] + y

    def project_step(j):
        @pl.when(r - 1 - j >= 0)
        def _():
            project(r - 1 - j, False)

        @pl.when(r + 1 + j < R)
        def _():
            project(r + 1 + j, False)

    project(r, True)

    @pl.loop(0, done_steps)
    def _(j):
        project_step(j)

    if done_steps < R - 1:
        @pl.loop(done_steps, R - 1)
        def _(j):
            line_step(j, w_all, w_up, w_dn, w_recv)

            @pl.when(j == R - 2)
            def _():
                start_o()

            project_step(j)
    else:
        start_o()

    def rope(x, cosine, sine):
        lane = lax.broadcasted_iota(jnp.int32, x.shape, 1)
        near = jnp.where(
            lane % HEAD_DIM < HEAD_DIM // 2,
            pltpu.roll(x, x.shape[1] - HEAD_DIM // 2, 1),
            pltpu.roll(x, HEAD_DIM // 2, 1),
        )
        return x * cosine + near * sine

    @pl.loop(0, rows // ptile)
    def _(b):
        at = pl.ds(pl.multiple_of(b * ptile, ptile), ptile)
        y = yacc[at, :]
        cosine = cos_ref[at, :]
        sine = sin_ref[at, :]
        kv[r, at, 0:128] = rope(y[:, 128:256], cosine, sine).astype(BF16)
        kv[r, at, 128:256] = y[:, 256:384].astype(BF16)
        p = y[:, 384:512].astype(BF16)
        pool[pl.ds(pl.multiple_of(TAIL + b * ptile, TAIL), ptile), :] = p.astype(F32)
        tail[...] = p[ptile - TAIL :, :]
        q = rope(y[:, 0:128], cosine, sine).astype(BF16) * jnp.array(HEAD_DIM**-0.5, BF16)
        lane = lax.broadcasted_iota(jnp.int32, q.shape, 1)
        zero = jnp.zeros_like(q)
        q_st[0, at, :] = jnp.where(lane < HEAD_DIM, q, zero)
        q_st[1, at, :] = jnp.where(lane >= HEAD_DIM, q, zero)

    def kv_copy(k):
        return rdma(kv.at[k], kv.at[k], kv_send.at[k], kv_recv.at[k], (s + G, t))

    tail_copy = rdma(tail, prior, pp_send, pp_recv, (s + G, t))

    @pl.when(has_up)
    def _():
        kv_copy(r).start()
        tail_copy.start()

    qtile = rows // 2

    def attend(k, diagonal):
        @pl.loop(0, 4)
        def _(b):
            m_index = b // 2
            at = pl.ds(pl.multiple_of((b % 2) * qtile, qtile), qtile)
            q = q_st[m_index, at, :]
            scores = lax.dot_general(
                q, kv[k, :, 0:128], (((1,), (1,)), ((), ())), preferred_element_type=F32
            )
            if diagonal:
                qpos = (b % 2) * qtile + lax.broadcasted_iota(jnp.int32, scores.shape, 0)
                kpos = lax.broadcasted_iota(jnp.int32, scores.shape, 1)
                scores = jnp.where(kpos <= qpos, scores, MASKED)
            top = jnp.max(scores, axis=-1, keepdims=True)
            if not diagonal:
                old = m_st[m_index, at, :]
                top = jnp.maximum(old, top)
                factor = jnp.exp(old - top)
            weights = jnp.exp(scores - top)
            total = jnp.sum(weights, axis=-1, keepdims=True)
            product = jnp.dot(weights.astype(BF16), kv[k, :, 128:256], preferred_element_type=F32)
            if not diagonal:
                total = total + l_st[m_index, at, :] * factor
                product = product + acc_st[m_index, at, :] * factor
            m_st[m_index, at, :] = top
            l_st[m_index, at, :] = total
            acc_st[m_index, at, :] = product

    attend(r, True)

    @pl.loop(0, R - 1)
    def _(j):
        k = r - 1 - j

        @pl.when(j < r)
        def _():
            kv_copy(k).wait_recv()

            @pl.when(has_up)
            def _():
                kv_copy(k).start()

        @pl.when(j > 0)
        def _():
            line_step(j - 1, o_all, o_up, o_dn, o_recv)

        @pl.when(j < r)
        def _():
            attend(k, False)

    @pl.when(has_dn)
    def _():
        tail_copy.wait_recv()
        pool[0:TAIL, :] = prior[...].astype(F32)

    @pl.when(r == 0)
    def _():
        pool[0:TAIL, :] = jnp.zeros((TAIL, GROUP_DIM), F32)

    ext = pool[...]
    kind = head % 4
    window = jnp.where(kind == 0, 2, jnp.where(kind == 1, 4, jnp.where(kind == 2, 8, 16)))
    run = ext + pltpu.roll(ext, 1, 0)
    chosen = run
    for power, lag in ((1, 2), (2, 4), (3, 8)):
        run = run + pltpu.roll(run, lag, 0)
        chosen = jnp.where(kind == power, run, chosen)
    spot = r * rows + lax.broadcasted_iota(jnp.int32, (rows, GROUP_DIM), 0)
    counts = jnp.minimum(spot + 1, window).astype(F32)
    mean = chosen[TAIL:, :] / counts - ext[TAIL:, :]
    mixedg = jnp.dot(mean.astype(BF16), gw_ref[head], preferred_element_type=F32)
    cat[:, 128:256] = (mixedg * ps_ref[head]).astype(BF16)

    diff = acc_st[0] / l_st[0] - lam_ref[head] * (acc_st[1] / l_st[1])
    inv = lax.rsqrt(jnp.mean(diff * diff, axis=-1, keepdims=True) + HEAD_FLOOR)
    cat[:, 0:128] = (diff * inv * hg_ref[...] * HEAD_SCALE).astype(BF16)

    share = rows // members
    half = part.shape[2]
    o_slots = o_all.shape[0] // CHUNKS
    by_line = R * PARTS == CHUNKS
    table = [sorted(range(R), key=lambda c: abs(c - i)) for i in range(R)]

    def chunk_at(k):
        if not by_line:
            return k
        total = 0
        for i in range(R):
            total = total + jnp.where(r == i, table[i][k // PARTS], 0)
        return total * PARTS + k % PARTS

    orders = ([t_bits[0], x_dim] + t_bits[1:], t_bits + [x_dim])

    def block(mask):
        gg, tt = member(mask)
        return pl.ds(pl.multiple_of((gg * TP + tt) * share, share), share)

    def combos(dims):
        found = [[]]
        for dim in dims:
            found = found + [mask + [dim] for mask in found]
        return found

    plans = []
    for h in range(CHUNKS):
        order = orders[h % 2]
        stages = []
        base = 0
        for i, dim in enumerate(order):
            masks = combos(order[i + 1 :])
            stages.append((dim, masks, base))
            base += len(masks)
        plans.append(stages)

    def rs_copy(h, dim, mask, index):
        at = block([dim] + mask)
        return rdma(
            sbuf.at[h, at, :], rbuf.at[h, index], rs_send.at[h, index], rs_recv.at[h, index],
            device([dim]),
        )

    def rs_start(h, i):
        dim, masks, base = plans[h][i]
        for n, mask in enumerate(masks):
            at = block([dim] + mask)
            sbuf[h, at, :] = part[h, at, :].astype(BF16)
        for n, mask in enumerate(masks):
            rs_copy(h, dim, mask, base + n).start()

    def rs_finish(h, i):
        dim, masks, base = plans[h][i]
        for n, mask in enumerate(masks):
            rs_copy(h, dim, mask, base + n).wait_recv()
            at = block(mask)
            part[h, at, :] = part[h, at, :] + rbuf[h, base + n].astype(F32)

    def out_product(h):
        first = chunk_at(h) * o_slots

        @pl.loop(0, 2)
        def _(b):
            at = pl.ds(pl.multiple_of(b * (rows // 2), rows // 2), rows // 2)
            columns = o_all[pl.ds(first, o_slots)].reshape(half, -1)
            part[h, at, :] = lax.dot_general(
                cat[at, :], columns, (((1,), (1,)), ((), ())), preferred_element_type=F32
            )

    levels = len(plans[0])
    mine = block([])
    last = lambda: line_step(R - 2, o_all, o_up, o_dn, o_recv)
    if by_line:
        batches = [range(CHUNKS - PARTS), range(CHUNKS - PARTS, CHUNKS)]
    else:
        batches = [range(CHUNKS)]
    def begin(batch):
        for h in batch:
            out_product(h)
            rs_start(h, 0)

    def advance(batch, i):
        for h in batch:
            rs_finish(h, i)
            if i + 1 < levels:
                rs_start(h, i + 1)
            else:
                at = pl.ds(pl.multiple_of(chunk_at(h) * half, half), half)
                out_ref[:, at] = part[h, mine, :].astype(BF16)

    if by_line:
        early, late = batches
        begin(early)
        advance(early, 0)
        last()
        begin(late)
        for i in range(1, levels):
            advance(early, i)
            advance(late, i - 1)
        advance(late, levels - 1)
    else:
        last()
        begin(batches[0])
        for i in range(levels):
            advance(batches[0], i)

    cross_copy(wp_ref, w_all, wx_send, w_recv).wait_send()
    cross_copy(op_ref, o_all, ox_send, o_recv).wait_send()
    drain(w_all, w_up, w_dn, w_recv)
    drain(o_all, o_up, o_dn, o_recv)
    for dim, stage in tok_stages:
        for mask, src, index in stage:
            tok_copy(dim, mask, src, index).wait_send()

    @pl.when(has_up)
    def _():
        tail_copy.wait_send()

        @pl.loop(0, r + 1)
        def _(k):
            kv_copy(k).wait_send()

    for h in range(CHUNKS):
        for dim, masks, base in plans[h]:
            for n, mask in enumerate(masks):
                rs_copy(h, dim, mask, base + n).wait_send()


def body(
    sp,
    tp,
    tokens,
    norm_gain,
    query_one,
    key_one,
    query_two,
    key_two,
    value_weight,
    pool_weight,
    lambda_head,
    head_gain,
    group_weight,
    pool_scale,
    out_attn,
    out_pool,
):
    G = query_one.shape[1] // HEAD_DIM
    assert G == 2 and sp % G == 0
    R = sp // G
    chunk, feats = tokens.shape
    rows = G * chunk
    depth = query_one.shape[0]
    cols = out_attn.shape[1]
    heads = lambda_head.shape[0]
    members = G * tp
    share = rows // members

    half_dim = HEAD_DIM // 2
    inverse = ROPE_BASE ** (-((np.arange(2 * HEAD_DIM) % half_dim) * 2.0 / HEAD_DIM))
    freq = jnp.asarray(inverse.astype(np.float32).reshape(1, -1))
    width = 4 * HEAD_DIM + VALUE_DIM + GROUP_DIM
    depth_out = VALUE_DIM + GROUP_DIM
    total_cols = sp * cols
    vm = pl.BlockSpec(memory_space=pltpu.VMEM)
    dma = pltpu.SemaphoreType.DMA
    return pl.pallas_call(
        functools.partial(kernel, (G, R, tp)),
        out_shape=jax.ShapeDtypeStruct((share, total_cols), BF16),
        in_specs=[vm] * 11 + [pl.BlockSpec(memory_space=pltpu.SMEM)] + [vm] * 3,
        out_specs=vm,
        scratch_shapes=[
            pltpu.VMEM((G, depth, width), BF16),
            pltpu.VMEM((G, cols, depth_out), BF16),
            pltpu.VMEM((rows, 2 * HEAD_DIM), F32),
            pltpu.VMEM((rows, 2 * HEAD_DIM), F32),
            pltpu.VMEM((rows, width), F32),
            pltpu.VMEM((G, tp, chunk, feats), BF16),
            pltpu.VMEM((R, rows, G * depth), BF16),
            pltpu.VMEM((sp, depth, width), BF16),
            pltpu.VMEM((sp, cols, depth_out), BF16),
            pltpu.VMEM((R, rows, 256), BF16),
            pltpu.VMEM((2, rows, 128), BF16),
            pltpu.VMEM((2, rows, 1), F32),
            pltpu.VMEM((2, rows, 1), F32),
            pltpu.VMEM((2, rows, VALUE_DIM), F32),
            pltpu.VMEM((TAIL + rows, GROUP_DIM), F32),
            pltpu.VMEM((TAIL, GROUP_DIM), BF16),
            pltpu.VMEM((TAIL, GROUP_DIM), BF16),
            pltpu.VMEM((rows, depth_out), BF16),
            pltpu.VMEM((CHUNKS, rows, total_cols // CHUNKS), F32),
            pltpu.VMEM((CHUNKS, rows, total_cols // CHUNKS), BF16),
            pltpu.VMEM((CHUNKS, members - 1, share, total_cols // CHUNKS), BF16),
            dma((members - 1,)),
            dma((members - 1,)),
            dma((sp,)),
            dma((sp,)),
            dma((sp,)),
            dma,
            dma((sp,)),
            dma((sp,)),
            dma((sp,)),
            dma,
            dma((R,)),
            dma((R,)),
            dma,
            dma,
            dma((CHUNKS, members - 1)),
            dma((CHUNKS, members - 1)),
        ],
        compiler_params=pltpu.CompilerParams(
            collective_id=0, has_side_effects=True, vmem_limit_bytes=58 * 1024 * 1024
        ),
    )(
        tokens,
        norm_gain.reshape(1, -1),
        query_one,
        key_one,
        query_two,
        key_two,
        value_weight,
        pool_weight,
        out_attn,
        out_pool,
        freq,
        lambda_head,
        head_gain.reshape(1, -1),
        group_weight,
        pool_scale.reshape(heads, 1, GROUP_DIM),
    )


def solution(mesh):
    in_specs = (
        P("sp", "tp"),
        P(),
        P("sp", "tp"),
        P("sp", "tp"),
        P("sp", "tp"),
        P("sp", "tp"),
        P("sp", "tp"),
        P("sp", "tp"),
        P(),
        P(),
        P(),
        P(),
        P("tp", "sp"),
        P("tp", "sp"),
    )
    return jax.shard_map(
        functools.partial(body, mesh.shape["sp"], mesh.shape["tp"]),
        mesh=mesh,
        in_specs=in_specs,
        out_specs=P(("sp", "tp"), None),
        check_vma=False,
    )
```
